256 devices in a mesh: sp: 64 (over z, y, core), tp: 4 (over x).
Axes of the slice: x: 4, y: 4, z: 8, core: 2. Of those that a mesh axis runs over, the one named last changes fastest.
Arguments:
- memory_queries: bfloat16 [16384, 768], P('sp', 'tp'), may hold values from -6 to 6
- memory_keys: bfloat16 [16384, 768], P('sp', 'tp'), may hold values from -6 to 6
- memory_values: bfloat16 [16384, 768], P('sp', 'tp'), may hold values from -6 to 6
- output_gate_preactivation: bfloat16 [16384, 768], P('sp', 'tp'), may hold values from -6 to 6
- log_input_gate: float32 [8, 16384], P('tp', 'sp'), may hold values from -4 to 300
- forget_preactivation: float32 [8, 16384], P('tp', 'sp'), may hold values from -5 to 5
- head_forget_bias: float32 [8], P('tp'), may hold values from 3 to 16
- forget_extra_boost: float32 [8, 16384], P('tp', 'sp'), may hold values from -2 to 0
- head_norm_gain: float32 [768], P('tp'), may hold values from 0.1 to 1.9
- memory_output_weight: bfloat16 [768, 2048], replicated, may hold values from -0.21875 to 0.21875
- residual: bfloat16 [16384, 2048], P('sp'), may hold values from -6 to 6
- expert_norm_gain: float32 [2048], replicated, may hold values from 0.1 to 1.9
- routes: int32 [16384, 4], P('sp'), may hold values from 0 to 255, all different within a row; in each aligned block of 256 rows (0 to 255, 256 to 511, ...) at most 8 rows name the same one
- router_weight_matrix: float32 [16384, 4], P('sp'), may hold values from 0.1 to 1
- routed_gate_weight: bfloat16 [256, 2048, 512], P('sp', None, 'tp'), may hold values from -0.125 to 0.125
- routed_up_weight: bfloat16 [256, 2048, 512], P('sp', None, 'tp'), may hold values from -0.125 to 0.125
- routed_down_weight: bfloat16 [256, 512, 2048], P('sp', 'tp'), may hold values from -0.25 to 0.25
- shared_gate_weight: bfloat16 [2048, 512], P(None, 'tp'), may hold values from -0.125 to 0.125
- shared_up_weight: bfloat16 [2048, 512], P(None, 'tp'), may hold values from -0.125 to 0.125
- shared_down_weight: bfloat16 [512, 2048], P('tp'), may hold values from -0.25 to 0.25
Outputs:
- updated: bfloat16 [16384, 2048], P('sp', 'tp')
The draws below stay inside these ranges and needn't reach their ends.
Inputs may be any that keep to these rules, and one draw needn't show every extreme that they name: `routes`: each row names 4 different experts. In each aligned block of 256 rows (the rows of one index of sp) no expert is named by more than 8 rows, a bound that some block reaches.
All inputs are finite; a program needn't handle non-finite values.
Results may differ from the reference program's by a relative error of at most 0.0085.
Values may be sent and summed in bfloat16 or wider, within the bound.
A program may use at most 128 MiB of HBM per device.

```python
import math
import jax
import jax.numpy as jnp
import numpy as np
from jax import lax

D = 2048
HEADS = 8
DH = 96
FF = 512
TOP_K = 4
TOK_DEV = 256
TOKENS = 16384
EXPERTS = 256
CAP = 8
N_SP = 64
N_TP = 4


def draw_log_input_gate(key, part):
    base = jnp.clip(jax.random.normal(jax.random.fold_in(key, 11), (HEADS, TOKENS), jnp.float32), -4.0, 4.0)
    return base


def draw_forget_preactivation(key, part):
    noise = jnp.clip(jax.random.normal(jax.random.fold_in(key, 21), (HEADS, TOKENS), jnp.float32), -4.0, 4.0)
    blocks = TOKENS // TOK_DEV
    offsets = jax.random.uniform(jax.random.fold_in(key, 22), (HEADS, blocks), jnp.float32, -0.7, 0.7)
    which = jnp.arange(TOKENS, dtype=jnp.int32) // TOK_DEV
    return noise + jnp.take(offsets, which, axis=1)


def draw_head_forget_bias(key, part):
    order = jax.random.permutation(jax.random.fold_in(key, 31), HEADS)
    fast = order < HEADS // 2
    jitter = jax.random.uniform(jax.random.fold_in(key, 32), (HEADS,), jnp.float32, -0.5, 0.5)
    return jnp.where(fast, jnp.log(40.0), jnp.log(4.0 * TOKENS)) + jitter


def draw_forget_extra_boost(key, part):
    spots = jax.random.randint(jax.random.fold_in(key, 41), (HEADS, 2), 0, TOKENS)
    losses = jnp.log(jax.random.uniform(jax.random.fold_in(key, 42), (HEADS, 2), jnp.float32, 0.5, 0.8))
    places = jnp.arange(TOKENS, dtype=jnp.int32)[None, None, :]
    return jnp.sum(jnp.where(places == spots[:, :, None], losses[:, :, None], 0.0), axis=1)


def shard_levels(stream_key, dims, pieces, smallest, top_value):
    factor_of, own = 1.0, jax.random.fold_in(stream_key, 6)
    for dim, blocks in pieces:
        draws = jnp.exp(jax.random.uniform(jax.random.fold_in(own, dim), (blocks,), jnp.float32, smallest / len(pieces), top_value / len(pieces)))
        factor_of = factor_of * jnp.repeat(draws, dims[dim] // blocks).reshape([-1 if axis == dim else 1 for axis in range(len(dims))])
    return factor_of


def deal_out(own_key, own, number, rows, number_of, top, most, skew):
    order = jax.random.permutation(own_key, number_of)
    crowded, ordinary = shares(number_of, rows * top, most, skew, True), shares(number_of, rows * top, most, skew, False)
    places = jnp.arange(number_of)

    def named(sizes, offset_by):
        used = int((sizes > 0).sum())
        fixed = max(1, used // 4)
        passed = fixed + (places - fixed + offset_by * (used - fixed)) % max(1, number_of - fixed)
        return jnp.zeros((number_of,), jnp.int32).at[order[jnp.where(places < fixed, places, passed)]].set(jnp.asarray(sizes, jnp.int32))

    sizes = jnp.where(number % 4 == 0, named(crowded, number // 4), named(ordinary, number - number // 4 - 1))
    mixed = jax.random.permutation(jax.random.fold_in(own, 3), number_of)
    giver, taker = mixed[0:number_of // 2 * 2:2], mixed[1:number_of // 2 * 2:2]
    margin = jnp.minimum(sizes[giver] - 1, most - sizes[taker]) // 2
    margin = jnp.where((giver == order[0]) | (taker == order[0]) | (sizes[taker] == 0), 0, jnp.maximum(margin, 0))
    passed = jax.random.randint(jax.random.fold_in(own, 4), (number_of // 2,), 0, 1 << 20) % (margin + 1)
    sizes = sizes.at[giver].add(-passed).at[taker].add(passed)
    items = jnp.searchsorted(jnp.cumsum(sizes), jnp.arange(rows * top), side="right").astype(jnp.int32)
    listing = items.reshape(top, rows).T
    listing = listing[jax.random.permutation(jax.random.fold_in(own, 1), rows)]
    offset_by = jax.random.randint(jax.random.fold_in(own, 2), (rows, 1), 0, top)
    return jnp.take_along_axis(listing, (jnp.arange(top)[None, :] + offset_by) % top, axis=1)


def shares(amount, total, bound, lean, full):
    portions = [(1 << 20) // math.isqrt(grade ** lean) + 1 for grade in range(1, amount + 1)]
    largest = bound if full else min(bound, max(-(-total // amount), total * portions[0] // sum(portions)))
    least = 1 if total - largest >= amount - 1 else 0
    given, rest = [largest] + [least] * (amount - 1), total - largest - least * (amount - 1)
    while rest > 0:
        free = [i for i in range(1, amount) if given[i] < largest] or [i for i in range(1, amount) if given[i] < bound]
        mass, remaining = sum([portions[i] for i in free]), rest
        for i in free:
            addition = min(bound - given[i], max(1, remaining * portions[i] // mass), rest)
            given[i] = given[i] + addition
            rest = rest - addition
    return np.array(given)


def bell_draw(key, shape, spread, bound, pieces=(), held_as=jnp.bfloat16):
    loudness = shard_levels(key, shape, pieces, -0.22, 0.18) if pieces else 1.0
    drawn = jax.random.normal(key, shape, jnp.float32) * spread * loudness
    return jnp.minimum(jnp.maximum(drawn, -bound), bound).astype(held_as)


def setup_inputs(seed: int = 0) -> dict:
    streams_of = jax.random.split(jax.random.key(seed), 21)
    memory_queries = bell_draw(streams_of[0], (TOKENS, HEADS * DH), 1.0, 6.0, ((0, 64), (1, 4)))
    memory_keys = bell_draw(streams_of[1], (TOKENS, HEADS * DH), 1.0, 6.0, ((0, 64), (1, 4)))
    memory_values = bell_draw(streams_of[2], (TOKENS, HEADS * DH), 1.0, 6.0, ((0, 64), (1, 4)))
    output_gate_preactivation = bell_draw(streams_of[3], (TOKENS, HEADS * DH), 1.0, 6.0, ((0, 64), (1, 4)))
    log_input_gate = draw_log_input_gate(jax.random.fold_in(streams_of[20], 71), 0)
    forget_preactivation = draw_forget_preactivation(jax.random.fold_in(streams_of[20], 71), 0)
    head_forget_bias = draw_head_forget_bias(jax.random.fold_in(streams_of[20], 71), 0)
    forget_extra_boost = draw_forget_extra_boost(jax.random.fold_in(streams_of[20], 71), 0)
    head_norm_gain = jnp.clip(1.0 + 0.18 * jax.random.normal(streams_of[8], (HEADS * DH,), jnp.float32), 0.1, 1.9)
    memory_output_weight = bell_draw(streams_of[9], (HEADS * DH, D), (HEADS * DH) ** -0.5, 0.21875)
    residual = bell_draw(streams_of[10], (TOKENS, D), 1.0, 6.0, ((0, 64),))
    expert_norm_gain = jnp.clip(1.0 + 0.18 * jax.random.normal(streams_of[11], (D,), jnp.float32), 0.1, 1.9)
    routes_keys = jax.random.split(jax.random.fold_in(streams_of[12], 1), TOKENS // TOK_DEV)
    routes_turns = jax.random.permutation(jax.random.fold_in(streams_of[12], 3), TOKENS // TOK_DEV)
    routes = jax.vmap(lambda own, number: deal_out(jax.random.fold_in(streams_of[12], 2), own, number, TOK_DEV, EXPERTS, TOP_K, CAP, 1))(routes_keys, routes_turns).reshape((TOKENS, TOP_K))
    router_weight_matrix = jnp.clip(jnp.exp(math.log(1.0) - 2.3025851 * jax.random.uniform(streams_of[13], (TOKENS, TOP_K), jnp.float32) ** shard_levels(streams_of[13], (TOKENS, TOP_K), ((0, 64),), -0.2, 0.2)), 0.1, 1.0)
    routed_gate_weight = bell_draw(streams_of[14], (EXPERTS, D, FF), D ** -0.5, 0.125, ((0, 64), (2, 4)))
    routed_up_weight = bell_draw(streams_of[15], (EXPERTS, D, FF), D ** -0.5, 0.125, ((0, 64), (2, 4)))
    routed_down_weight = bell_draw(streams_of[16], (EXPERTS, FF, D), FF ** -0.5, 0.25, ((0, 64), (1, 4)))
    shared_gate_weight = bell_draw(streams_of[17], (D, FF), D ** -0.5, 0.125, ((1, 4),))
    shared_up_weight = bell_draw(streams_of[18], (D, FF), D ** -0.5, 0.125, ((1, 4),))
    shared_down_weight = bell_draw(streams_of[19], (FF, D), FF ** -0.5, 0.25, ((0, 4),))
    return dict(memory_queries=memory_queries, memory_keys=memory_keys, memory_values=memory_values, output_gate_preactivation=output_gate_preactivation, log_input_gate=log_input_gate, forget_preactivation=forget_preactivation, head_forget_bias=head_forget_bias, forget_extra_boost=forget_extra_boost, head_norm_gain=head_norm_gain, memory_output_weight=memory_output_weight, residual=residual, expert_norm_gain=expert_norm_gain, routes=routes, router_weight_matrix=router_weight_matrix, routed_gate_weight=routed_gate_weight, routed_up_weight=routed_up_weight, routed_down_weight=routed_down_weight, shared_gate_weight=shared_gate_weight, shared_up_weight=shared_up_weight, shared_down_weight=shared_down_weight)


NEG_LARGE = -1e+30
EPSILON = 1e-06

def matrix_memory_cell(memory_queries, memory_keys, memory_values, output_gate_preactivation, log_input_gate, forget_preactivation, head_forget_bias, forget_extra_boost, head_norm_gain):
    blocks = TOKENS // TOK_DEV
    scale = DH ** (-0.5)
    queries = memory_queries.reshape(blocks, TOK_DEV, HEADS, DH)
    keyset = memory_keys.reshape(blocks, TOK_DEV, HEADS, DH)
    valueset = memory_values.reshape(blocks, TOK_DEV, HEADS, DH)
    forget_log_gate = jax.nn.log_sigmoid(forget_preactivation + head_forget_bias[:, None]) + forget_extra_boost
    forget_log_gate = forget_log_gate.reshape(HEADS, blocks, TOK_DEV).transpose(1, 0, 2)
    log_input = log_input_gate.reshape(HEADS, blocks, TOK_DEV).transpose(1, 0, 2)
    causal = jnp.tril(jnp.ones((TOK_DEV, TOK_DEV), bool))

    def advance(carry, inputs):
        memory, stabil = carry
        q_block, k_block, v_block, i_block, f_block = inputs
        cumul = jnp.cumsum(f_block, axis=1)
        d_log = jnp.where(causal[None], cumul[:, :, None] - cumul[:, None, :] + i_block[:, None, :], NEG_LARGE)
        g_log = cumul + stabil[:, None]
        top = jnp.maximum(g_log, lax.optimization_barrier(jnp.max(d_log, axis=2)))
        q_float = q_block.astype(jnp.float32)
        k_float = k_block.astype(jnp.float32)
        v_float = v_block.astype(jnp.float32)
        scores = jnp.einsum('thd,shd->hts', q_float, k_float, precision=lax.Precision.HIGHEST) * scale
        weights = scores * jnp.exp(d_log - top[:, :, None])
        rounded = lax.optimization_barrier(weights.astype(jnp.bfloat16)).astype(jnp.float32)
        inter = jnp.exp(g_log - top)
        q_scaled = q_float * scale
        numer = jnp.einsum('hts,shd->thd', rounded, v_float, precision=lax.Precision.HIGHEST)
        hidden = numer + inter.T[:, :, None] * jnp.einsum('thd,hde->the', q_scaled, memory, precision=lax.Precision.HIGHEST)
        ending = cumul[:, -1]
        w_log = ending[:, None] - cumul + i_block
        new_top = jnp.maximum(ending + stabil, lax.optimization_barrier(jnp.max(w_log, axis=1)))
        w_end = jnp.exp(w_log - new_top[:, None])
        decay = jnp.exp(ending + stabil - new_top)
        memory = decay[:, None, None] * memory + jnp.einsum('hs,shd,she->hde', w_end, k_float, v_float, precision=lax.Precision.HIGHEST)
        return ((memory, new_top), hidden)
    start = (jnp.zeros((HEADS, DH, DH), jnp.float32), jnp.full((HEADS,), NEG_LARGE, jnp.float32))
    _, hiddens = lax.scan(advance, start, (queries, keyset, valueset, log_input, forget_log_gate))
    hiddens = hiddens.reshape(TOKENS, HEADS, DH)
    hiddens = hiddens * lax.rsqrt(lax.optimization_barrier(jnp.mean(hiddens * hiddens, axis=2, keepdims=True)) + EPSILON)
    gated = hiddens.reshape(TOKENS, HEADS * DH) * head_norm_gain * jax.nn.sigmoid(output_gate_preactivation.astype(jnp.float32))
    return gated.astype(jnp.bfloat16)

def reference(memory_queries, memory_keys, memory_values, output_gate_preactivation, log_input_gate, forget_preactivation, head_forget_bias, forget_extra_boost, head_norm_gain, memory_output_weight, residual, expert_norm_gain, routes, router_weight_matrix, routed_gate_weight, routed_up_weight, routed_down_weight, shared_gate_weight, shared_up_weight, shared_down_weight):
    token_mixing = matrix_memory_cell(memory_queries, memory_keys, memory_values, output_gate_preactivation, log_input_gate, forget_preactivation, head_forget_bias, forget_extra_boost, head_norm_gain)
    stream = residual.astype(jnp.float32) + jnp.dot(token_mixing, memory_output_weight, preferred_element_type=jnp.float32)
    normed = (stream * lax.rsqrt(lax.optimization_barrier(jnp.mean(stream * stream, axis=1, keepdims=True)) + EPSILON) * expert_norm_gain).astype(jnp.bfloat16)
    group = FF // N_TP
    most_rows = N_SP * CAP
    flat_routes = routes.reshape(-1)
    flat_owner = jnp.arange(TOKENS * TOP_K, dtype=jnp.int32) // TOP_K
    flat_weight = router_weight_matrix.reshape(-1)
    order = jnp.argsort(flat_routes, stable=True)
    sorted_owner = jnp.concatenate([flat_owner[order], jnp.zeros((most_rows,), jnp.int32)])
    sorted_weight = jnp.concatenate([flat_weight[order], jnp.zeros((most_rows,), jnp.float32)])
    counts = jnp.bincount(flat_routes, length=EXPERTS).astype(jnp.int32)
    starts = (jnp.cumsum(counts) - counts).astype(jnp.int32)
    lanes = jnp.arange(most_rows, dtype=jnp.int32)

    def one_expert(total, expert):
        valid = lanes < counts[expert]
        owners = lax.dynamic_slice(sorted_owner, (starts[expert],), (most_rows,))
        weights = lax.dynamic_slice(sorted_weight, (starts[expert],), (most_rows,))
        owners = jnp.where(valid, owners, 0).astype(jnp.int32)
        weights = jnp.where(valid, weights, 0.0)
        picked = normed[owners]
        gate_vals = jnp.dot(picked, routed_gate_weight[expert], preferred_element_type=jnp.float32)
        up_vals = jnp.dot(picked, routed_up_weight[expert], preferred_element_type=jnp.float32)
        hidden = (jax.nn.silu(gate_vals) * up_vals).astype(jnp.bfloat16)
        hidden_groups = hidden.reshape(most_rows, N_TP, group).astype(jnp.float32)
        down_groups = routed_down_weight[expert].reshape(N_TP, group, D).astype(jnp.float32)
        partials = jnp.einsum('rjf,jfd->rjd', hidden_groups, down_groups, precision=lax.Precision.HIGHEST)
        partials = partials.astype(jnp.bfloat16).astype(jnp.float32)
        output = lax.optimization_barrier(jnp.sum(partials, axis=1)).astype(jnp.bfloat16).astype(jnp.float32)
        return (total.at[owners].add(weights[:, None] * output), None)
    routed, _ = lax.scan(one_expert, jnp.zeros((TOKENS, D), jnp.float32), jnp.arange(EXPERTS, dtype=jnp.int32))
    shared_hidden = (jax.nn.silu(jnp.dot(normed, shared_gate_weight, preferred_element_type=jnp.float32)) * jnp.dot(normed, shared_up_weight, preferred_element_type=jnp.float32)).astype(jnp.bfloat16)
    shared = jnp.zeros((TOKENS, D), jnp.float32)
    for index in range(N_TP):
        piece = jnp.dot(shared_hidden[:, index * group:(index + 1) * group], shared_down_weight[index * group:(index + 1) * group], preferred_element_type=jnp.float32)
        shared = shared + piece.astype(jnp.bfloat16).astype(jnp.float32)
    return (stream + routed + shared).astype(jnp.bfloat16)
```

```python
import jax
import jax.numpy as jnp
from jax import lax
from jax.experimental import pallas as pl
from jax.experimental.pallas import tpu as pltpu
from jax.sharding import Mesh
from jax.sharding import PartitionSpec as P

SP = ("sp_0", "sp_1", "sp_2")
MESH_ID = pl.DeviceIdType.MESH
NEG_LARGE = -1e30
EPSILON = 1e-06
F32 = jnp.float32
BF16 = jnp.bfloat16
HIGHEST = lax.Precision.HIGHEST

NZ, NY, NC, NX = 8, 4, 2, 4
PLANE = NY * NC
N_SP = NZ * PLANE
TOK = 256
DH = 96
HW = 192
D = 2048
FF = 512
GROUP = FF // NX
CAP = 8
SLOTS = N_SP * CAP
NEAR = PLANE * NX * CAP
LANES = 128
SLICE = HW // PLANE
QUARTER = D // NX
CHUNK = 2 * PLANE


def nt(a, b, precision=None):
    return lax.dot_general(
        a, b, (((1,), (1,)), ((), ())), preferred_element_type=F32, precision=precision
    )


def tn(a, b, precision=None):
    return lax.dot_general(
        a, b, (((0,), (0,)), ((), ())), preferred_element_type=F32, precision=precision
    )


def nn(a, b, precision=None):
    return jnp.dot(a, b, preferred_element_type=F32, precision=precision)


def arrival(ref, sem):
    pltpu.make_async_copy(ref, ref, sem).wait()


def z_offset(i):
    return jnp.where(lax.rem(i, 2) == 0, 4 + i // 2, 4 - (i + 1) // 2)


def kernel(
    q_hbm,
    k_hbm,
    v_hbm,
    og_hbm,
    lig_hbm,
    fpre_hbm,
    bias_ref,
    boost_hbm,
    hgain_ref,
    wo_hbm,
    res_hbm,
    egain_ref,
    routes_hbm,
    rw_hbm,
    gate_hbm,
    up_hbm,
    down_hbm,
    sg_hbm,
    su_hbm,
    sd_hbm,
    out_ref,
    q_ref,
    k_ref,
    v_ref,
    og_ref,
    lig_ref,
    fpre_ref,
    boost_ref,
    wo_ref,
    res_ref,
    routes_ref,
    rw_ref,
    sg_ref,
    su_ref,
    sd_ref,
    wg_ref,
    wu_ref,
    wd_ref,
    state_ref,
    plane_ref,
    zst_ref,
    fin_ref,
    carry_ref,
    mix_ref,
    mixed_ref,
    hidden_ref,
    stream_ref,
    normed_ref,
    pick_ref,
    whi_ref,
    wlo_ref,
    shared_ref,
    sbuf_ref,
    rbuf_ref,
    eo_ref,
    near_ref,
    rs_ref,
    chain_out_ref,
    chain_in_ref,
    table_ref,
    in_sem,
    own_sem,
    wsend_sem,
    wrecv_sem,
    st_send,
    st_recv,
    mix_send,
    mix_recv,
    d_send,
    d_recv,
    b_send,
    b_recv,
    rs_ssem,
    rs_rsem,
    chain_send,
    chain_recv,
):
    z, y, c, x = (lax.axis_index(a) for a in ("sp_0", "sp_1", "sp_2", "tp"))
    p = y * NC + c
    sp = z * PLANE + p

    def sp_dev(tz, tp_):
        return {"sp_0": tz, "sp_1": tp_ // NC, "sp_2": lax.rem(tp_, NC)}

    early = (
        (lig_hbm, lig_ref),
        (fpre_hbm, fpre_ref),
        (boost_hbm, boost_ref),
        (k_hbm, k_ref),
        (v_hbm, v_ref),
        (q_hbm, q_ref),
        (og_hbm, og_ref),
        (routes_hbm, routes_ref),
        (rw_hbm, rw_ref),
        (wo_hbm, wo_ref),
        (res_hbm, res_ref),
        (sg_hbm, sg_ref),
        (su_hbm, su_ref),
        (sd_hbm, sd_ref),
    )
    loads = [pltpu.make_async_copy(a, b, in_sem.at[n]) for n, (a, b) in enumerate(early)]
    for cp in loads:
        cp.start()

    barrier = pltpu.get_barrier_semaphore()

    @pl.loop(1, N_SP)
    def _(n):
        pl.semaphore_signal(
            barrier,
            inc=1,
            device_id=sp_dev(lax.rem(z + n // PLANE, NZ), lax.rem(p + n, PLANE)),
            device_id_type=MESH_ID,
        )

    @pl.loop(0, (NX - 1) * PLANE)
    def _(n):
        pl.semaphore_signal(
            barrier,
            inc=1,
            device_id={
                **sp_dev(z, lax.rem(p + n, PLANE)),
                "tp": lax.rem(x + 1 + n // PLANE, NX),
            },
            device_id_type=MESH_ID,
        )

    own_weights = (
        pltpu.make_async_copy(
            gate_hbm.at[x], wg_ref.at[:, pl.ds(pl.multiple_of(x * GROUP, GROUP), GROUP)], own_sem.at[0]
        ),
        pltpu.make_async_copy(
            up_hbm.at[x], wu_ref.at[:, pl.ds(pl.multiple_of(x * GROUP, GROUP), GROUP)], own_sem.at[1]
        ),
        pltpu.make_async_copy(
            down_hbm.at[x], wd_ref.at[pl.ds(pl.multiple_of(x * GROUP, GROUP), GROUP)], own_sem.at[2]
        ),
    )

    for n in range(3):
        loads[n].wait()
    second = lax.broadcasted_iota(jnp.int32, (2, TOK), 0) == 1
    bias = jnp.where(second, bias_ref[1], bias_ref[0])
    pre = fpre_ref[...] + bias
    log_forget = jnp.minimum(pre, 0.0) - jnp.log1p(jnp.exp(-jnp.abs(pre))) + boost_ref[...]
    row = lax.broadcasted_iota(jnp.int32, (TOK, TOK), 0)
    col = lax.broadcasted_iota(jnp.int32, (TOK, TOK), 1)
    causal = row <= col
    upper = jnp.where(causal, 1.0, 0.0).astype(F32)
    eye = jnp.where(row == col, 1.0, 0.0).astype(F32)
    log_in = lig_ref[...]
    cumul = nn(log_forget, upper, HIGHEST)
    source = nt(eye, log_in - cumul, HIGHEST)
    ending = jnp.sum(log_forget, axis=1, keepdims=True)
    w_log = ending - cumul + log_in
    local_top = jnp.max(w_log, axis=1, keepdims=True)
    w_end = jnp.exp(w_log - local_top)

    loads[3].wait()
    loads[4].wait()
    lane = lax.broadcasted_iota(jnp.int32, (DH, LANES), 1)
    slice_lane = lax.broadcasted_iota(jnp.int32, (SLICE, LANES), 1)

    def with_scalars(mem, top, total, lanes):
        return jnp.where(lanes == DH, top, jnp.where(lanes == DH + 1, total, mem))

    def taken_apart(block):
        return block, block[:, DH : DH + 1], block[:, DH + 1 : DH + 2]

    padding = jnp.zeros((LANES - DH, TOK), F32)
    for h in range(2):
        keys = k_ref[h * DH : (h + 1) * DH].astype(F32) * w_end[h : h + 1]
        values = v_ref[h * DH : (h + 1) * DH].astype(F32)
        memory = nt(values, jnp.concatenate([keys, padding], axis=0), HIGHEST)
        state = with_scalars(memory, local_top[h : h + 1], ending[h : h + 1], lane)
        state_ref[h * (PLANE // 2) : (h + 1) * (PLANE // 2)] = state.reshape(PLANE // 2, SLICE, LANES)

    pl.semaphore_wait(barrier, N_SP - 1 + (NX - 1) * PLANE)

    @pl.loop(1, PLANE)
    def _(n):
        to = lax.rem(p + n, PLANE)
        pltpu.make_async_remote_copy(
            state_ref.at[to],
            plane_ref.at[p],
            st_send.at[0],
            st_recv.at[0],
            device_id=sp_dev(z, to),
            device_id_type=MESH_ID,
        ).start()

    own_rows = pl.ds(pl.multiple_of(x * GROUP, GROUP), GROUP)

    def send_weights(n, src, dst):
        for step in (1, 3, 2):
            to = lax.rem(x + step, NX)
            pltpu.make_async_remote_copy(
                src(to),
                dst,
                wsend_sem.at[n],
                wrecv_sem.at[n],
                device_id={"tp": to},
                device_id_type=MESH_ID,
            ).start()

    upper_half, lower_half = pl.ds(0, D // 2), pl.ds(D // 2, D // 2)
    send_weights(0, lambda to: gate_hbm.at[to, upper_half], wg_ref.at[upper_half, own_rows])
    for cp in own_weights:
        cp.start()
    plane_ref[p] = state_ref[p]

    loads[5].wait()
    scale = DH ** (-0.5)
    local_max, numer = [], []
    for h in range(2):
        head = slice(h * DH, (h + 1) * DH)
        d_log = jnp.where(causal, cumul[h : h + 1] + source[:, h : h + 1], NEG_LARGE)
        top = jnp.max(d_log, axis=0, keepdims=True)
        scores = tn(k_ref[head], q_ref[head]) * scale
        within = (scores * jnp.exp(d_log - top)).astype(BF16)
        numer.append(nn(v_ref[head], within))
        local_max.append(top)

    def join(earlier, later):
        mem_a, top_a, total_a = earlier
        mem_b, top_b, total_b = later
        top = jnp.maximum(total_b + top_a, top_b)
        mem = jnp.exp(total_b + top_a - top) * mem_a + jnp.exp(top_b - top) * mem_b
        return mem, top, total_a + total_b

    none = (
        jnp.zeros((SLICE, LANES), F32),
        jnp.full((SLICE, 1), NEG_LARGE, F32),
        jnp.zeros((SLICE, 1), F32),
    )
    arrival(plane_ref.at[pl.ds(0, PLANE - 1)], st_recv.at[0])
    whole, before = none, []
    for n in range(PLANE):
        before.append(whole)
        whole = join(whole, taken_apart(plane_ref[n]))
    zst_ref[z] = with_scalars(*whole, slice_lane)

    @pl.loop(1, NZ)
    def _(n):
        pltpu.make_async_remote_copy(
            zst_ref.at[z],
            zst_ref.at[z],
            st_send.at[1],
            st_recv.at[1],
            device_id={"sp_0": lax.rem(z + n, NZ)},
            device_id_type=MESH_ID,
        ).start()

    loads[7].wait()
    loads[8].wait()
    table_ref[z] = jnp.concatenate([routes_ref[...].astype(F32), rw_ref[...]], axis=0)

    @pl.loop(1, NZ)
    def _(n):
        pltpu.make_async_remote_copy(
            table_ref.at[z],
            table_ref.at[z],
            st_send.at[3],
            st_recv.at[3],
            device_id={"sp_0": lax.rem(z + n, NZ)},
            device_id_type=MESH_ID,
        ).start()

    slot = lax.broadcasted_iota(jnp.int32, (SLOTS, TOK), 0)
    expert = slot // CAP * NX + x
    named = jnp.zeros((SLOTS, TOK), F32)
    for n in range(4):
        named = jnp.where(routes_ref[n : n + 1] == expert, 1.0, named)
    strict = jnp.where(row < col, 1.0, 0.0).astype(BF16)
    rank = nn(named.astype(BF16), strict)
    pick_ref[...] = jnp.where(rank == lax.rem(slot, CAP).astype(F32), named, 0.0).astype(BF16)
    hgain = nt(eye[:HW, :HW], hgain_ref[...], HIGHEST)
    loads[6].wait()
    gating = hgain * jax.nn.sigmoid(og_ref[...].astype(F32))

    arrival(zst_ref.at[pl.ds(0, NZ - 1)], st_recv.at[1])
    carried = none
    for n in range(NZ):
        mem, top, total = taken_apart(zst_ref[n])
        passed = n < z
        carried = join(
            carried, (mem, jnp.where(passed, top, NEG_LARGE), jnp.where(passed, total, 0.0))
        )
    z_mem, z_top, z_total = carried
    z_mem = jnp.where(z > 0, z_mem, 0.0)
    for n in range(PLANE):
        fin_ref[n] = with_scalars(*join((z_mem, z_top, z_total), before[n]), slice_lane)

    @pl.loop(1, PLANE)
    def _(n):
        to = lax.rem(p + n, PLANE)
        pltpu.make_async_remote_copy(
            fin_ref.at[to],
            carry_ref.at[p],
            st_send.at[2],
            st_recv.at[2],
            device_id=sp_dev(z, to),
            device_id_type=MESH_ID,
        ).start()

    carry_ref[p] = fin_ref[p]
    arrival(carry_ref.at[pl.ds(0, PLANE - 1)], st_recv.at[2])
    no_queries = jnp.zeros((LANES - DH, TOK), BF16)
    for h in range(2):
        head = slice(h * DH, (h + 1) * DH)
        memory = carry_ref[h * (PLANE // 2) : (h + 1) * (PLANE // 2)].reshape(DH, LANES)
        carry_top = memory[0:1, DH : DH + 1]
        memory = jnp.where(lane < DH, memory, 0.0)
        high = memory.astype(BF16)
        low = (memory - high.astype(F32)).astype(BF16)
        queries = jnp.concatenate([q_ref[head], no_queries], axis=0)
        inter = nn(high, queries) + nn(low, queries)
        g_log = cumul[h : h + 1] + carry_top
        stab = jnp.maximum(g_log, local_max[h])
        cell = numer[h] * jnp.exp(local_max[h] - stab) + inter * (jnp.exp(g_log - stab) * scale)
        mean = jnp.sum(cell * cell, axis=0, keepdims=True) / DH
        mix_ref[x, head] = (cell * lax.rsqrt(mean + EPSILON) * gating[head]).astype(BF16)
    for step in (1, 3, 2):
        pltpu.make_async_remote_copy(
            mix_ref.at[x],
            mix_ref.at[x],
            mix_send,
            mix_recv,
            device_id={"tp": lax.rem(x + step, NX)},
            device_id_type=MESH_ID,
        ).start()
    send_weights(0, lambda to: gate_hbm.at[to, lower_half], wg_ref.at[lower_half, own_rows])
    send_weights(1, lambda to: up_hbm.at[to], wu_ref.at[:, own_rows])
    send_weights(2, lambda to: down_hbm.at[to], wd_ref.at[own_rows])

    loads[9].wait()
    loads[10].wait()
    arrival(mix_ref.at[pl.ds(0, NX - 1)], mix_recv)
    mixed_ref[...] = jnp.transpose(mix_ref[...].astype(F32).reshape(NX * HW, TOK)).astype(BF16)

    def project(n, total):
        columns = pl.ds(pl.multiple_of(n * QUARTER, QUARTER), QUARTER)
        part = res_ref[:, columns].astype(F32) + nn(mixed_ref[...], wo_ref[:, columns])
        stream_ref[n] = part
        return total + jnp.sum(part * part, axis=1, keepdims=True)

    square = lax.fori_loop(0, NX, project, jnp.zeros((TOK, 1), F32))
    inverse = lax.rsqrt(square / D + EPSILON)

    @pl.loop(0, NX)
    def _(n):
        columns = pl.ds(pl.multiple_of(n * QUARTER, QUARTER), QUARTER)
        normed_ref[:, columns] = (stream_ref[n] * inverse * egain_ref[:, columns]).astype(BF16)

    @pl.loop(0, NZ)
    def _(i):
        to_z = lax.rem(z + z_offset(i), NZ)
        chosen = pick_ref[pl.ds(pl.multiple_of(to_z * PLANE * CAP, PLANE * CAP), PLANE * CAP)]
        rows = nn(chosen, normed_ref[...])
        sbuf_ref[pl.ds(i * PLANE, PLANE)] = rows.reshape(PLANE, CAP, D).astype(BF16)

        @pl.loop(0, PLANE)
        def _(n):
            to = lax.rem(p + n, PLANE)
            itself = (i == NZ - 1) & (n == 0)

            @pl.when(jnp.logical_not(itself))
            def _():
                pltpu.make_async_remote_copy(
                    sbuf_ref.at[i * PLANE + to],
                    rbuf_ref.at[i * PLANE + p],
                    d_send,
                    d_recv.at[i],
                    device_id=sp_dev(to_z, to),
                    device_id_type=MESH_ID,
                ).start()

            @pl.when(itself)
            def _():
                pltpu.make_async_copy(
                    sbuf_ref.at[i * PLANE + to], rbuf_ref.at[i * PLANE + p], d_recv.at[i]
                ).start()

    for n in range(11, 14):
        loads[n].wait()
    normed = normed_ref[...]
    shared_hidden = (jax.nn.silu(nn(normed, sg_ref[...])) * nn(normed, su_ref[...])).astype(BF16)
    for n in range(NX):
        shared_ref[n] = nn(shared_hidden, sd_ref[:, n * QUARTER : (n + 1) * QUARTER]).astype(BF16)

    arrival(table_ref.at[pl.ds(0, NZ - 1)], st_recv.at[3])
    slot = lax.broadcasted_iota(jnp.int32, (NEAR, TOK), 0)
    expert = (slot // CAP + z * (PLANE * NX)).astype(F32)
    place = lax.rem(slot, CAP).astype(F32)

    @pl.loop(0, NZ)
    def _(n):
        table = table_ref[n]
        named = jnp.zeros((NEAR, TOK), F32)
        weight = jnp.zeros((NEAR, TOK), F32)
        for k in range(4):
            hit = table[k : k + 1] == expert
            named = jnp.where(hit, 1.0, named)
            weight = jnp.where(hit, table[k + 4 : k + 5], weight)
        rank = nn(named.astype(BF16), strict)
        weight = jnp.transpose(jnp.where(rank == place, weight, 0.0))
        high = weight.astype(BF16)
        whi_ref[n] = high
        wlo_ref[n] = (weight - high.astype(F32)).astype(BF16)

    for cp in own_weights:
        cp.wait()
    arrival(wg_ref.at[:, pl.ds(0, FF - GROUP)], wrecv_sem.at[0])
    arrival(wu_ref.at[:, pl.ds(0, FF - GROUP)], wrecv_sem.at[1])

    @pl.loop(0, NZ // 2)
    def _(s):
        arrival(rbuf_ref.at[pl.ds(0, PLANE)], d_recv.at[2 * s])
        arrival(rbuf_ref.at[pl.ds(0, PLANE)], d_recv.at[2 * s + 1])
        blocks = pl.ds(pl.multiple_of(s * CHUNK, CHUNK), CHUNK)
        rows = rbuf_ref[blocks].astype(F32).reshape(CHUNK * CAP, D).astype(BF16)
        hidden = jax.nn.silu(nn(rows, wg_ref[...])) * nn(rows, wu_ref[...])
        hidden_ref[s] = hidden.astype(BF16)

    arrival(wd_ref.at[pl.ds(0, FF - GROUP)], wrecv_sem.at[2])

    @pl.loop(0, NZ // 2)
    def _(s):
        for n in range(NX):
            result = nn(hidden_ref[s], wd_ref[:, n * QUARTER : (n + 1) * QUARTER])
            result = result.reshape(2, PLANE, CAP, QUARTER).astype(BF16)
            for k in range(2):
                eo_ref[s, n, :, k] = result[k]

        @pl.loop(0, NX * PLANE)
        def _(n):
            to, to_x = lax.rem(p + n // NX, PLANE), lax.rem(x + n, NX)

            @pl.when(n > 0)
            def _():
                pltpu.make_async_remote_copy(
                    eo_ref.at[s, to_x, to],
                    near_ref.at[s, p * NX + x],
                    b_send,
                    b_recv.at[s],
                    device_id={**sp_dev(z, to), "tp": to_x},
                    device_id_type=MESH_ID,
                ).start()

            @pl.when(n == 0)
            def _():
                pltpu.make_async_copy(
                    eo_ref.at[s, to_x, to], near_ref.at[s, p * NX + x], b_recv.at[s]
                ).start()

    for step in (1, 3, 2):
        to = lax.rem(x + step, NX)
        pltpu.make_async_remote_copy(
            shared_ref.at[to],
            rs_ref.at[x],
            rs_ssem,
            rs_rsem,
            device_id={"tp": to},
            device_id_type=MESH_ID,
        ).start()

    width = QUARTER // 2

    def weighted(i, h):
        block = lax.rem(z + NZ - z_offset(i), NZ)
        rows = near_ref[i // 2, :, i % 2, :, h * width : (h + 1) * width]
        rows = rows.astype(F32).reshape(NEAR, width).astype(BF16)
        return nn(whi_ref[block], rows) + nn(wlo_ref[block], rows)

    def arrived(i, h):
        arrival(chain_in_ref.at[2 * i + h], chain_recv.at[2 * i + h])
        return chain_in_ref[2 * i + h].astype(F32)

    def passed_on(i, h, before, up):
        part = weighted(i, h)
        if before is not None:
            part = part + arrived(before, h)
        chain_out_ref[2 * i + h] = part.astype(BF16)
        pltpu.make_async_remote_copy(
            chain_out_ref.at[2 * i + h],
            chain_in_ref.at[2 * i + h],
            chain_send,
            chain_recv.at[2 * i + h],
            device_id={"sp_0": lax.rem(z + (1 if up else NZ - 1), NZ)},
            device_id_type=MESH_ID,
        ).start()

    arrival(near_ref.at[0], b_recv.at[0])
    passed_on(0, 0, None, True)
    passed_on(0, 1, None, False)
    passed_on(1, 0, None, False)
    arrival(near_ref.at[1], b_recv.at[1])
    passed_on(2, 1, None, True)
    passed_on(1, 1, 0, False)
    passed_on(2, 0, 0, True)
    passed_on(3, 0, 1, False)
    arrival(near_ref.at[2], b_recv.at[2])
    passed_on(4, 1, 2, True)
    passed_on(3, 1, 1, False)
    passed_on(4, 0, 2, True)
    passed_on(5, 0, 3, False)
    arrival(near_ref.at[3], b_recv.at[3])
    passed_on(6, 1, 4, True)
    passed_on(5, 1, 3, False)
    passed_on(6, 0, 4, True)

    rs_ref[x] = shared_ref[x]
    arrival(rs_ref.at[pl.ds(0, NX - 1)], rs_rsem)
    totals = []
    for h in range(2):
        columns = slice(h * width, (h + 1) * width)
        total = stream_ref[x, :, columns] + weighted(NZ - 1, h)
        for n in range(NX):
            total = total + rs_ref[n, :, columns].astype(F32)
        totals.append(total)
    for h in range(2):
        total = totals[h] + arrived(5, h) + arrived(6, h)
        out_ref[:, h * width : (h + 1) * width] = total.astype(BF16)

    arrival(plane_ref.at[pl.ds(0, PLANE - 1)], st_send.at[0])
    arrival(zst_ref.at[pl.ds(0, NZ - 1)], st_send.at[1])
    arrival(fin_ref.at[pl.ds(0, PLANE - 1)], st_send.at[2])
    arrival(mix_ref.at[pl.ds(0, NX - 1)], mix_send)
    arrival(wg_ref.at[:, pl.ds(0, FF - GROUP)], wsend_sem.at[0])
    arrival(wu_ref.at[:, pl.ds(0, FF - GROUP)], wsend_sem.at[1])
    arrival(wd_ref.at[pl.ds(0, FF - GROUP)], wsend_sem.at[2])
    arrival(sbuf_ref.at[pl.ds(0, N_SP - 1)], d_send)
    arrival(table_ref.at[pl.ds(0, NZ - 1)], st_send.at[3])
    for n in range(NZ // 2):
        arrival(near_ref.at[n, pl.ds(0, NX * PLANE - 1)], b_send)
    arrival(rs_ref.at[pl.ds(0, NX - 1)], rs_ssem)
    arrival(chain_out_ref, chain_send)


def body(
    memory_queries,
    memory_keys,
    memory_values,
    output_gate_preactivation,
    log_input_gate,
    forget_preactivation,
    head_forget_bias,
    forget_extra_boost,
    head_norm_gain,
    memory_output_weight,
    residual,
    expert_norm_gain,
    routes,
    router_weight_matrix,
    routed_gate_weight,
    routed_up_weight,
    routed_down_weight,
    shared_gate_weight,
    shared_up_weight,
    shared_down_weight,
):
    anywhere = pl.BlockSpec(memory_space=pl.ANY)
    vmem = pl.BlockSpec(memory_space=pltpu.VMEM)
    smem = pl.BlockSpec(memory_space=pltpu.SMEM)
    specs = [anywhere] * 20
    specs[6] = smem
    specs[8] = vmem
    specs[11] = vmem
    dma = pltpu.SemaphoreType.DMA
    return pl.pallas_call(
        kernel,
        out_shape=jax.ShapeDtypeStruct((TOK, QUARTER), BF16),
        in_specs=specs,
        out_specs=vmem,
        scratch_shapes=[
            pltpu.VMEM((HW, TOK), BF16),
            pltpu.VMEM((HW, TOK), BF16),
            pltpu.VMEM((HW, TOK), BF16),
            pltpu.VMEM((HW, TOK), BF16),
            pltpu.VMEM((2, TOK), F32),
            pltpu.VMEM((2, TOK), F32),
            pltpu.VMEM((2, TOK), F32),
            pltpu.VMEM((NX * HW, D), BF16),
            pltpu.VMEM((TOK, D), BF16),
            pltpu.VMEM((4, TOK), jnp.int32),
            pltpu.VMEM((4, TOK), F32),
            pltpu.VMEM((D, GROUP), BF16),
            pltpu.VMEM((D, GROUP), BF16),
            pltpu.VMEM((GROUP, D), BF16),
            pltpu.VMEM((D, FF), BF16),
            pltpu.VMEM((D, FF), BF16),
            pltpu.VMEM((FF, D), BF16),
            pltpu.VMEM((PLANE, SLICE, LANES), F32),
            pltpu.VMEM((PLANE, SLICE, LANES), F32),
            pltpu.VMEM((NZ, SLICE, LANES), F32),
            pltpu.VMEM((PLANE, SLICE, LANES), F32),
            pltpu.VMEM((PLANE, SLICE, LANES), F32),
            pltpu.VMEM((NX, HW, TOK), BF16),
            pltpu.VMEM((TOK, NX * HW), BF16),
            pltpu.VMEM((NZ // 2, CHUNK * CAP, FF), BF16),
            pltpu.VMEM((NX, TOK, QUARTER), F32),
            pltpu.VMEM((TOK, D), BF16),
            pltpu.VMEM((SLOTS, TOK), BF16),
            pltpu.VMEM((NZ, TOK, NEAR), BF16),
            pltpu.VMEM((NZ, TOK, NEAR), BF16),
            pltpu.VMEM((NX, TOK, QUARTER), BF16),
            pltpu.VMEM((N_SP, CAP, D), BF16),
            pltpu.VMEM((N_SP, CAP, D), BF16),
            pltpu.VMEM((NZ // 2, NX, PLANE, 2, CAP, QUARTER), BF16),
            pltpu.VMEM((NZ // 2, NX * PLANE, 2, CAP, QUARTER), BF16),
            pltpu.VMEM((NX, TOK, QUARTER), BF16),
            pltpu.VMEM((14, TOK, QUARTER // 2), BF16),
            pltpu.VMEM((14, TOK, QUARTER // 2), BF16),
            pltpu.VMEM((NZ, 8, TOK), F32),
            dma((14,)),
            dma((3,)),
            dma((3,)),
            dma((3,)),
            dma((4,)),
            dma((4,)),
            dma,
            dma,
            dma,
            dma((NZ,)),
            dma,
            dma((NZ // 2,)),
            dma,
            dma,
            dma,
            dma((14,)),
        ],
        compiler_params=pltpu.CompilerParams(
            collective_id=0, has_side_effects=True, vmem_limit_bytes=60 << 20
        ),
        name="layer",
    )(
        memory_queries.T,
        memory_keys.T,
        memory_values.T,
        output_gate_preactivation.T,
        log_input_gate,
        forget_preactivation,
        head_forget_bias,
        forget_extra_boost,
        head_norm_gain.reshape(1, HW),
        memory_output_weight,
        residual,
        expert_norm_gain.reshape(1, D),
        routes.T,
        router_weight_matrix.T,
        routed_gate_weight,
        routed_up_weight,
        routed_down_weight,
        shared_gate_weight,
        shared_up_weight,
        shared_down_weight,
    )


def solution(mesh):
    split = Mesh(
        mesh.devices.reshape(NZ, NY, NC, mesh.shape["tp"]), ("sp_0", "sp_1", "sp_2", "tp")
    )
    return jax.shard_map(
        body,
        mesh=split,
        in_specs=(
            P(SP, "tp"),
            P(SP, "tp"),
            P(SP, "tp"),
            P(SP, "tp"),
            P("tp", SP),
            P("tp", SP),
            P("tp"),
            P("tp", SP),
            P("tp"),
            P(),
            P(SP, None),
            P(),
            P(SP, None),
            P(SP, None),
            P(SP, None, "tp"),
            P(SP, None, "tp"),
            P(SP, "tp", None),
            P(None, "tp"),
            P(None, "tp"),
            P("tp", None),
        ),
        out_specs=P(SP, "tp"),
        check_vma=False,
    )
```

```python
import jax
import jax.numpy as jnp
from jax import lax
from jax.experimental import pallas as pl
from jax.experimental.pallas import tpu as pltpu
from jax.sharding import Mesh
from jax.sharding import PartitionSpec as P

SP = ("sp_0", "sp_1", "sp_2")
MESH_ID = pl.DeviceIdType.MESH
NEG_LARGE = -1e30
EPSILON = 1e-06
F32 = jnp.float32
BF16 = jnp.bfloat16
HIGHEST = lax.Precision.HIGHEST

NZ, NY, NC, NX = 8, 4, 2, 4
PLANE = NY * NC
N_SP = NZ * PLANE
TOK = 256
DH = 96
HW = 192
D = 2048
FF = 512
GROUP = FF // NX
CAP = 8
SLOTS = N_SP * CAP
NEAR = PLANE * NX * CAP
LANES = 128
SOON = 1024
SLICE = HW // PLANE
QUARTER = D // NX
CHUNK = 2 * PLANE


def nt(a, b, precision=None):
    return lax.dot_general(
        a, b, (((1,), (1,)), ((), ())), preferred_element_type=F32, precision=precision
    )


def tn(a, b, precision=None):
    return lax.dot_general(
        a, b, (((0,), (0,)), ((), ())), preferred_element_type=F32, precision=precision
    )


def nn(a, b, precision=None):
    return jnp.dot(a, b, preferred_element_type=F32, precision=precision)


def arrival(ref, sem):
    pltpu.make_async_copy(ref, ref, sem).wait()


def z_offset(i):
    return jnp.where(lax.rem(i, 2) == 0, 4 + i // 2, 4 - (i + 1) // 2)


def kernel(
    q_hbm,
    k_hbm,
    v_hbm,
    og_hbm,
    lig_hbm,
    fpre_hbm,
    bias_ref,
    boost_hbm,
    hgain_ref,
    wo_hbm,
    res_hbm,
    egain_ref,
    routes_hbm,
    rw_hbm,
    gate_hbm,
    up_hbm,
    down_hbm,
    sg_hbm,
    su_hbm,
    sd_hbm,
    out_ref,
    q_ref,
    k_ref,
    v_ref,
    og_ref,
    lig_ref,
    fpre_ref,
    boost_ref,
    wo_ref,
    res_ref,
    routes_ref,
    rw_ref,
    sg_ref,
    su_ref,
    sd_ref,
    wg_ref,
    wu_ref,
    wd_ref,
    state_ref,
    plane_ref,
    zst_ref,
    fin_ref,
    carry_ref,
    mix_ref,
    mixed_ref,
    hidden_ref,
    stream_ref,
    normed_ref,
    pick_ref,
    whi_ref,
    wlo_ref,
    shared_ref,
    sbuf_ref,
    rbuf_ref,
    eo_ref,
    near_ref,
    chain_out_ref,
    chain_in_ref,
    table_ref,
    in_sem,
    own_sem,
    wsend_sem,
    wrecv_sem,
    st_send,
    st_recv,
    mix_send,
    mix_recv,
    d_send,
    d_recv,
    b_send,
    b_recv,
    rs_ssem,
    rs_rsem,
    chain_send,
    chain_recv,
    swap_send,
    swap_recv,
):
    z, y, c, x = (lax.axis_index(a) for a in ("sp_0", "sp_1", "sp_2", "tp"))
    p = y * NC + c
    sp = z * PLANE + p

    def sp_dev(tz, tp_):
        return {"sp_0": tz, "sp_1": tp_ // NC, "sp_2": lax.rem(tp_, NC)}

    own_rows = pl.ds(pl.multiple_of(x * GROUP, GROUP), GROUP)

    def quarter_of(n):
        return pl.ds(pl.multiple_of(n * QUARTER, QUARTER), QUARTER)

    early = (
        (lig_hbm, lig_ref),
        (fpre_hbm, fpre_ref),
        (boost_hbm, boost_ref),
        (k_hbm, k_ref),
        (v_hbm, v_ref),
        (q_hbm, q_ref),
        (og_hbm, og_ref),
        (routes_hbm, routes_ref),
        (rw_hbm, rw_ref),
        (wo_hbm, wo_ref),
        (res_hbm, res_ref),
        (sg_hbm, sg_ref),
        (su_hbm, su_ref),
        (sd_hbm.at[:, quarter_of(x)], sd_ref.at[own_rows]),
    )
    loads = [pltpu.make_async_copy(a, b, in_sem.at[n]) for n, (a, b) in enumerate(early)]
    for cp in loads:
        cp.start()

    barrier = pltpu.get_barrier_semaphore()

    @pl.loop(1, NZ)
    def _(n):
        pl.semaphore_signal(
            barrier, inc=1, device_id={"sp_0": lax.rem(z + n, NZ)}, device_id_type=MESH_ID
        )

    @pl.loop(1, NX * PLANE)
    def _(n):
        pl.semaphore_signal(
            barrier,
            inc=1,
            device_id={
                **sp_dev(z, lax.rem(p + n, PLANE)),
                "tp": lax.rem(x + n // PLANE, NX),
            },
            device_id_type=MESH_ID,
        )

    own_weights = (
        pltpu.make_async_copy(
            gate_hbm.at[x], wg_ref.at[:, own_rows], own_sem.at[0]
        ),
        pltpu.make_async_copy(
            up_hbm.at[x], wu_ref.at[:, own_rows], own_sem.at[1]
        ),
        pltpu.make_async_copy(
            down_hbm.at[x], wd_ref.at[own_rows], own_sem.at[2]
        ),
    )

    for n in range(3):
        loads[n].wait()
    second = lax.broadcasted_iota(jnp.int32, (2, TOK), 0) == 1
    bias = jnp.where(second, bias_ref[1], bias_ref[0])
    pre = fpre_ref[...] + bias
    log_forget = jnp.minimum(pre, 0.0) - jnp.log1p(jnp.exp(-jnp.abs(pre))) + boost_ref[...]
    row = lax.broadcasted_iota(jnp.int32, (TOK, TOK), 0)
    col = lax.broadcasted_iota(jnp.int32, (TOK, TOK), 1)
    causal = row <= col
    upper = jnp.where(causal, 1.0, 0.0).astype(F32)
    eye = jnp.where(row == col, 1.0, 0.0).astype(F32)
    log_in = lig_ref[...]
    cumul = nn(log_forget, upper, HIGHEST)
    source = nt(eye, log_in - cumul, HIGHEST)
    ending = jnp.sum(log_forget, axis=1, keepdims=True)
    w_log = ending - cumul + log_in
    local_top = jnp.max(w_log, axis=1, keepdims=True)
    w_end = jnp.exp(w_log - local_top)

    loads[3].wait()
    loads[4].wait()
    lane = lax.broadcasted_iota(jnp.int32, (DH, LANES), 1)
    slice_lane = lax.broadcasted_iota(jnp.int32, (SLICE, LANES), 1)

    def with_scalars(mem, top, total, lanes):
        return jnp.where(lanes == DH, top, jnp.where(lanes == DH + 1, total, mem))

    def taken_apart(block):
        return block, block[:, DH : DH + 1], block[:, DH + 1 : DH + 2]

    padding = jnp.zeros((LANES - DH, TOK), F32)
    for h in range(2):
        keys = k_ref[h * DH : (h + 1) * DH].astype(F32) * w_end[h : h + 1]
        values = v_ref[h * DH : (h + 1) * DH].astype(F32)
        memory = nt(values, jnp.concatenate([keys, padding], axis=0), HIGHEST)
        state = with_scalars(memory, local_top[h : h + 1], ending[h : h + 1], lane)
        state_ref[h * (PLANE // 2) : (h + 1) * (PLANE // 2)] = state.reshape(PLANE // 2, SLICE, LANES)

    pl.semaphore_wait(barrier, NZ - 1 + NX * PLANE - 1)

    @pl.loop(1, PLANE)
    def _(n):
        to = lax.rem(p + n, PLANE)
        pltpu.make_async_remote_copy(
            state_ref.at[to],
            plane_ref.at[p],
            st_send.at[0],
            st_recv.at[0],
            device_id=sp_dev(z, to),
            device_id_type=MESH_ID,
        ).start()

    def send_weights(n, src, dst):
        for step in (2, 1, 3):
            to = lax.rem(x + step, NX)
            pltpu.make_async_remote_copy(
                src(to),
                dst,
                wsend_sem.at[n],
                wrecv_sem.at[n],
                device_id={"tp": to},
                device_id_type=MESH_ID,
            ).start()

    upper_half, lower_half = pl.ds(0, SOON), pl.ds(SOON, D - SOON)
    def core_rows(k):
        start = pl.multiple_of(k * GROUP + c * (GROUP // NC), GROUP // NC)
        return pl.ds(start, GROUP // NC)

    send_weights(
        3,
        lambda to: sd_hbm.at[
            pl.ds(pl.multiple_of(c * (GROUP // NC), GROUP // NC), GROUP // NC),
            quarter_of(to),
        ],
        sd_ref.at[core_rows(x)],
    )
    send_weights(0, lambda to: gate_hbm.at[to, upper_half], wg_ref.at[upper_half, own_rows])
    for cp in own_weights:
        cp.start()
    plane_ref[p] = state_ref[p]

    loads[5].wait()
    scale = DH ** (-0.5)
    local_max, numer = [], []
    for h in range(2):
        head = slice(h * DH, (h + 1) * DH)
        d_log = jnp.where(causal, cumul[h : h + 1] + source[:, h : h + 1], NEG_LARGE)
        top = jnp.max(d_log, axis=0, keepdims=True)
        scores = tn(k_ref[head], q_ref[head]) * scale
        within = (scores * jnp.exp(d_log - top)).astype(BF16)
        numer.append(nn(v_ref[head], within))
        local_max.append(top)

    def join(earlier, later):
        mem_a, top_a, total_a = earlier
        mem_b, top_b, total_b = later
        top = jnp.maximum(total_b + top_a, top_b)
        mem = jnp.exp(total_b + top_a - top) * mem_a + jnp.exp(top_b - top) * mem_b
        return mem, top, total_a + total_b

    none = (
        jnp.zeros((SLICE, LANES), F32),
        jnp.full((SLICE, 1), NEG_LARGE, F32),
        jnp.zeros((SLICE, 1), F32),
    )
    arrival(plane_ref.at[pl.ds(0, PLANE - 1)], st_recv.at[0])
    whole, before = none, []
    for n in range(PLANE):
        before.append(whole)
        whole = join(whole, taken_apart(plane_ref[n]))
    zst_ref[z] = with_scalars(*whole, slice_lane)

    @pl.loop(1, NZ)
    def _(n):
        pltpu.make_async_remote_copy(
            zst_ref.at[z],
            zst_ref.at[z],
            st_send.at[1],
            st_recv.at[1],
            device_id={"sp_0": lax.rem(z + n, NZ)},
            device_id_type=MESH_ID,
        ).start()

    loads[7].wait()
    loads[8].wait()
    table_ref[z] = jnp.concatenate([routes_ref[...].astype(F32), rw_ref[...]], axis=0)

    @pl.loop(1, NZ)
    def _(n):
        pltpu.make_async_remote_copy(
            table_ref.at[z],
            table_ref.at[z],
            st_send.at[3],
            st_recv.at[3],
            device_id={"sp_0": lax.rem(z + n, NZ)},
            device_id_type=MESH_ID,
        ).start()

    slot = lax.broadcasted_iota(jnp.int32, (SLOTS, TOK), 0)
    expert = slot // CAP * NX + x
    named = jnp.zeros((SLOTS, TOK), F32)
    for n in range(4):
        named = jnp.where(routes_ref[n : n + 1] == expert, 1.0, named)
    strict = jnp.where(row < col, 1.0, 0.0).astype(BF16)
    rank = nn(named.astype(BF16), strict)
    pick_ref[...] = jnp.where(rank == lax.rem(slot, CAP).astype(F32), named, 0.0).astype(BF16)
    hgain = nt(eye[:HW, :HW], hgain_ref[...], HIGHEST)
    loads[6].wait()
    gating = hgain * jax.nn.sigmoid(og_ref[...].astype(F32))

    arrival(zst_ref.at[pl.ds(0, NZ - 1)], st_recv.at[1])
    carried = none
    for n in range(NZ):
        mem, top, total = taken_apart(zst_ref[n])
        passed = n < z
        carried = join(
            carried, (mem, jnp.where(passed, top, NEG_LARGE), jnp.where(passed, total, 0.0))
        )
    z_mem, z_top, z_total = carried
    z_mem = jnp.where(z > 0, z_mem, 0.0)
    for n in range(PLANE):
        fin_ref[n] = with_scalars(*join((z_mem, z_top, z_total), before[n]), slice_lane)

    @pl.loop(1, PLANE)
    def _(n):
        to = lax.rem(p + n, PLANE)
        pltpu.make_async_remote_copy(
            fin_ref.at[to],
            carry_ref.at[p],
            st_send.at[2],
            st_recv.at[2],
            device_id=sp_dev(z, to),
            device_id_type=MESH_ID,
        ).start()

    carry_ref[p] = fin_ref[p]
    arrival(carry_ref.at[pl.ds(0, PLANE - 1)], st_recv.at[2])
    no_queries = jnp.zeros((LANES - DH, TOK), BF16)
    for h in range(2):
        head = slice(h * DH, (h + 1) * DH)
        memory = carry_ref[h * (PLANE // 2) : (h + 1) * (PLANE // 2)].reshape(DH, LANES)
        carry_top = memory[0:1, DH : DH + 1]
        memory = jnp.where(lane < DH, memory, 0.0)
        high = memory.astype(BF16)
        low = (memory - high.astype(F32)).astype(BF16)
        queries = jnp.concatenate([q_ref[head], no_queries], axis=0)
        inter = nn(high, queries) + nn(low, queries)
        g_log = cumul[h : h + 1] + carry_top
        stab = jnp.maximum(g_log, local_max[h])
        cell = numer[h] * jnp.exp(local_max[h] - stab) + inter * (jnp.exp(g_log - stab) * scale)
        mean = jnp.sum(cell * cell, axis=0, keepdims=True) / DH
        mix_ref[x, head] = (cell * lax.rsqrt(mean + EPSILON) * gating[head]).astype(BF16)
    for step in (1, 3, 2):
        pltpu.make_async_remote_copy(
            mix_ref.at[x],
            mix_ref.at[x],
            mix_send,
            mix_recv,
            device_id={"tp": lax.rem(x + step, NX)},
            device_id_type=MESH_ID,
        ).start()
    send_weights(0, lambda to: gate_hbm.at[to, lower_half], wg_ref.at[lower_half, own_rows])
    send_weights(1, lambda to: up_hbm.at[to], wu_ref.at[:, own_rows])
    for j in (0, 1, 3, 2):
        for step in (2, 1, 3):
            to = lax.rem(x + step, NX)
            columns = quarter_of(lax.rem(to + j, NX))
            pltpu.make_async_remote_copy(
                down_hbm.at[to, :, columns],
                wd_ref.at[own_rows, columns],
                wsend_sem.at[2],
                wrecv_sem.at[4 if j == 2 else 2],
                device_id={"tp": to},
                device_id_type=MESH_ID,
            ).start()

    loads[9].wait()
    loads[10].wait()
    arrival(mix_ref.at[pl.ds(0, NX - 1)], mix_recv)
    mixed_ref[...] = jnp.transpose(mix_ref[...].astype(F32).reshape(NX * HW, TOK)).astype(BF16)

    def project(n, total):
        columns = quarter_of(n)
        part = res_ref[:, columns].astype(F32) + nn(mixed_ref[...], wo_ref[:, columns])
        stream_ref[n] = part
        return total + jnp.sum(part * part, axis=1, keepdims=True)

    square = lax.fori_loop(0, NX, project, jnp.zeros((TOK, 1), F32))
    inverse = lax.rsqrt(square / D + EPSILON)

    @pl.loop(0, NX)
    def _(n):
        columns = quarter_of(n)
        normed_ref[:, columns] = (stream_ref[n] * inverse * egain_ref[:, columns]).astype(BF16)

    @pl.loop(0, NZ)
    def _(i):
        to_z = lax.rem(z + z_offset(i), NZ)
        chosen = pick_ref[pl.ds(pl.multiple_of(to_z * PLANE * CAP, PLANE * CAP), PLANE * CAP)]
        rows = nn(chosen, normed_ref[...])
        sbuf_ref[pl.ds(i * PLANE, PLANE)] = rows.reshape(PLANE, CAP, D).astype(BF16)

        @pl.loop(0, PLANE)
        def _(n):
            to = lax.rem(p + n, PLANE)
            itself = (i == NZ - 1) & (n == 0)

            @pl.when(jnp.logical_not(itself))
            def _():
                pltpu.make_async_remote_copy(
                    sbuf_ref.at[i * PLANE + to],
                    rbuf_ref.at[i * PLANE + p],
                    d_send,
                    d_recv.at[i],
                    device_id=sp_dev(to_z, to),
                    device_id_type=MESH_ID,
                ).start()

            @pl.when(itself)
            def _():
                pltpu.make_async_copy(
                    sbuf_ref.at[i * PLANE + to], rbuf_ref.at[i * PLANE + p], d_recv.at[i]
                ).start()

    arrival(sd_ref.at[pl.ds(0, (NX - 1) * (GROUP // NC))], wrecv_sem.at[3])
    for step in range(1, NX):
        rows = core_rows(lax.rem(x + step, NX))
        pltpu.make_async_remote_copy(
            sd_ref.at[rows],
            sd_ref.at[rows],
            swap_send,
            swap_recv,
            device_id={"sp_2": 1 - c},
            device_id_type=MESH_ID,
        ).start()
    for n in range(11, 14):
        loads[n].wait()
    normed = normed_ref[...]
    shared_hidden = jax.nn.silu(nn(normed, sg_ref[...])) * nn(normed, su_ref[...])
    shared_ref[:, own_rows] = shared_hidden.astype(BF16)

    arrival(table_ref.at[pl.ds(0, NZ - 1)], st_recv.at[3])
    slot = lax.broadcasted_iota(jnp.int32, (NEAR, TOK), 0)
    expert = (slot // CAP + z * (PLANE * NX)).astype(F32)
    place = lax.rem(slot, CAP).astype(F32)

    @pl.loop(0, NZ)
    def _(n):
        table = table_ref[n]
        named = jnp.zeros((NEAR, TOK), F32)
        weight = jnp.zeros((NEAR, TOK), F32)
        for k in range(4):
            hit = table[k : k + 1] == expert
            named = jnp.where(hit, 1.0, named)
            weight = jnp.where(hit, table[k + 4 : k + 5], weight)
        rank = nn(named.astype(BF16), strict)
        weight = jnp.transpose(jnp.where(rank == place, weight, 0.0))
        high = weight.astype(BF16)
        whi_ref[n] = high
        wlo_ref[n] = (weight - high.astype(F32)).astype(BF16)

    for cp in own_weights:
        cp.wait()
    arrival(wg_ref.at[:, pl.ds(0, FF - GROUP)], wrecv_sem.at[0])
    arrival(wu_ref.at[:, pl.ds(0, FF - GROUP)], wrecv_sem.at[1])

    @pl.loop(0, NZ // 2)
    def _(s):
        arrival(rbuf_ref.at[pl.ds(0, PLANE)], d_recv.at[2 * s])
        arrival(rbuf_ref.at[pl.ds(0, PLANE)], d_recv.at[2 * s + 1])
        blocks = pl.ds(pl.multiple_of(s * CHUNK, CHUNK), CHUNK)
        rows = rbuf_ref[blocks].astype(F32).reshape(CHUNK * CAP, D).astype(BF16)
        hidden = jax.nn.silu(nn(rows, wg_ref[...])) * nn(rows, wu_ref[...])
        hidden_ref[s] = hidden.astype(BF16)

    arrival(wd_ref.at[pl.ds(0, FF - GROUP), pl.ds(0, D - QUARTER)], wrecv_sem.at[2])

    def send_back(src, dst, sem, columns):
        for j in columns:
            to_x = lax.rem(x + j, NX)

            @pl.loop(0 if j else 1, PLANE)
            def _(n):
                to = lax.rem(p + n, PLANE)
                pltpu.make_async_remote_copy(
                    src(to_x, to),
                    dst,
                    b_send,
                    sem,
                    device_id={**sp_dev(z, to), "tp": to_x},
                    device_id_type=MESH_ID,
                ).start()

            if j == 0:
                pltpu.make_async_copy(src(x, p), dst, sem).start()

    def out_of_expert(s, k, rows, columns):
        for j in columns:
            n = lax.rem(x + j, NX)
            result = nn(rows, wd_ref[:, quarter_of(n)])
            result = result.reshape(-1, PLANE, CAP, QUARTER).astype(BF16)
            for m in range(result.shape[0]):
                eo_ref[s, n, :, k + m] = result[m]

    def both_back(s, columns):
        out_of_expert(s, 0, hidden_ref[s], columns)
        send_back(
            lambda to_x, to: eo_ref.at[s, to_x, to],
            near_ref.at[s, p * NX + x],
            b_recv.at[2 * s],
            columns,
        )

    def one_back(i, columns):
        s, k = i // 2, i % 2
        rows = hidden_ref[s, k * (PLANE * CAP) : (k + 1) * (PLANE * CAP)]
        out_of_expert(s, k, rows, columns)
        send_back(
            lambda to_x, to: eo_ref.at[s, to_x, to, k],
            near_ref.at[s, p * NX + x, k],
            b_recv.at[i],
            columns,
        )

    width = QUARTER // 2

    def weighted(i, h):
        block = lax.rem(z + NZ - z_offset(i), NZ)
        rows = near_ref[i // 2, :, i % 2, :, h * width : (h + 1) * width]
        rows = rows.astype(F32).reshape(NEAR, width).astype(BF16)
        return nn(whi_ref[block], rows) + nn(wlo_ref[block], rows)

    def arrived(i, h):
        arrival(chain_in_ref.at[2 * i + h], chain_recv.at[2 * i + h])
        return chain_in_ref[2 * i + h].astype(F32)

    def passed_on(i, h, before, up):
        part = weighted(i, h)
        if before is not None:
            part = part + arrived(before, h)
        chain_out_ref[2 * i + h] = part.astype(BF16)
        pltpu.make_async_remote_copy(
            chain_out_ref.at[2 * i + h],
            chain_in_ref.at[2 * i + h],
            chain_send,
            chain_recv.at[2 * i + h],
            device_id={"sp_0": lax.rem(z + (1 if up else NZ - 1), NZ)},
            device_id_type=MESH_ID,
        ).start()

    soon, every = (1, 3, 0), (2, 1, 3, 0)
    one_back(0, soon)
    one_back(1, soon)
    arrival(wd_ref.at[pl.ds(0, FF - GROUP), pl.ds(0, QUARTER)], wrecv_sem.at[4])
    one_back(0, (2,))
    one_back(1, (2,))
    both_back(1, every)
    both_back(2, every)
    arrival(near_ref.at[0, :, 0], b_recv.at[0])
    passed_on(0, 0, None, True)
    passed_on(0, 1, None, False)
    arrival(near_ref.at[0, :, 1], b_recv.at[1])
    passed_on(1, 0, None, False)
    one_back(6, every)
    arrival(near_ref.at[1], b_recv.at[2])
    passed_on(2, 1, None, True)
    passed_on(2, 0, 0, True)
    passed_on(1, 1, 0, False)
    one_back(7, every)
    for step in (2, 1, 3):
        pltpu.make_async_remote_copy(
            shared_ref.at[:, own_rows],
            shared_ref.at[:, own_rows],
            rs_ssem,
            rs_rsem,
            device_id={"tp": lax.rem(x + step, NX)},
            device_id_type=MESH_ID,
        ).start()
    passed_on(3, 0, 1, False)
    arrival(near_ref.at[2], b_recv.at[4])
    passed_on(4, 1, 2, True)
    passed_on(3, 1, 1, False)
    passed_on(4, 0, 2, True)
    passed_on(5, 0, 3, False)
    arrival(near_ref.at[3, :, 0], b_recv.at[6])
    passed_on(6, 1, 4, True)
    passed_on(5, 1, 3, False)
    passed_on(6, 0, 4, True)

    arrival(near_ref.at[3, :, 1], b_recv.at[7])
    totals = []
    for h in range(2):
        totals.append(stream_ref[x, :, h * width : (h + 1) * width] + weighted(NZ - 1, h))
    arrival(sd_ref.at[pl.ds(0, (NX - 1) * (GROUP // NC))], swap_recv)
    arrival(shared_ref.at[:, pl.ds(0, FF - GROUP)], rs_rsem)
    for h in range(2):
        columns = slice(h * width, (h + 1) * width)
        total = totals[h] + nn(shared_ref[...], sd_ref[:, columns])
        total = total + arrived(5, h) + arrived(6, h)
        out_ref[:, columns] = total.astype(BF16)

    arrival(plane_ref.at[pl.ds(0, PLANE - 1)], st_send.at[0])
    arrival(zst_ref.at[pl.ds(0, NZ - 1)], st_send.at[1])
    arrival(fin_ref.at[pl.ds(0, PLANE - 1)], st_send.at[2])
    arrival(mix_ref.at[pl.ds(0, NX - 1)], mix_send)
    arrival(wg_ref.at[:, pl.ds(0, FF - GROUP)], wsend_sem.at[0])
    arrival(wu_ref.at[:, pl.ds(0, FF - GROUP)], wsend_sem.at[1])
    arrival(wd_ref.at[pl.ds(0, FF - GROUP)], wsend_sem.at[2])
    arrival(sbuf_ref.at[pl.ds(0, N_SP - 1)], d_send)
    arrival(table_ref.at[pl.ds(0, NZ - 1)], st_send.at[3])
    for n in range(NZ // 2):
        arrival(near_ref.at[n, pl.ds(0, NX * PLANE - 1)], b_send)
    arrival(sd_ref.at[pl.ds(0, (NX - 1) * (GROUP // NC))], wsend_sem.at[3])
    arrival(sd_ref.at[pl.ds(0, (NX - 1) * (GROUP // NC))], swap_send)
    arrival(shared_ref.at[:, pl.ds(0, FF - GROUP)], rs_ssem)
    arrival(chain_out_ref, chain_send)


def body(
    memory_queries,
    memory_keys,
    memory_values,
    output_gate_preactivation,
    log_input_gate,
    forget_preactivation,
    head_forget_bias,
    forget_extra_boost,
    head_norm_gain,
    memory_output_weight,
    residual,
    expert_norm_gain,
    routes,
    router_weight_matrix,
    routed_gate_weight,
    routed_up_weight,
    routed_down_weight,
    shared_gate_weight,
    shared_up_weight,
    shared_down_weight,
):
    anywhere = pl.BlockSpec(memory_space=pl.ANY)
    vmem = pl.BlockSpec(memory_space=pltpu.VMEM)
    smem = pl.BlockSpec(memory_space=pltpu.SMEM)
    specs = [anywhere] * 20
    specs[6] = smem
    specs[8] = vmem
    specs[11] = vmem
    dma = pltpu.SemaphoreType.DMA
    return pl.pallas_call(
        kernel,
        out_shape=jax.ShapeDtypeStruct((TOK, QUARTER), BF16),
        in_specs=specs,
        out_specs=vmem,
        scratch_shapes=[
            pltpu.VMEM((HW, TOK), BF16),
            pltpu.VMEM((HW, TOK), BF16),
            pltpu.VMEM((HW, TOK), BF16),
            pltpu.VMEM((HW, TOK), BF16),
            pltpu.VMEM((2, TOK), F32),
            pltpu.VMEM((2, TOK), F32),
            pltpu.VMEM((2, TOK), F32),
            pltpu.VMEM((NX * HW, D), BF16),
            pltpu.VMEM((TOK, D), BF16),
            pltpu.VMEM((4, TOK), jnp.int32),
            pltpu.VMEM((4, TOK), F32),
            pltpu.VMEM((D, GROUP), BF16),
            pltpu.VMEM((D, GROUP), BF16),
            pltpu.VMEM((FF, QUARTER), BF16),
            pltpu.VMEM((D, FF), BF16),
            pltpu.VMEM((D, FF), BF16),
            pltpu.VMEM((FF, D), BF16),
            pltpu.VMEM((PLANE, SLICE, LANES), F32),
            pltpu.VMEM((PLANE, SLICE, LANES), F32),
            pltpu.VMEM((NZ, SLICE, LANES), F32),
            pltpu.VMEM((PLANE, SLICE, LANES), F32),
            pltpu.VMEM((PLANE, SLICE, LANES), F32),
            pltpu.VMEM((NX, HW, TOK), BF16),
            pltpu.VMEM((TOK, NX * HW), BF16),
            pltpu.VMEM((NZ // 2, CHUNK * CAP, FF), BF16),
            pltpu.VMEM((NX, TOK, QUARTER), F32),
            pltpu.VMEM((TOK, D), BF16),
            pltpu.VMEM((SLOTS, TOK), BF16),
            pltpu.VMEM((NZ, TOK, NEAR), BF16),
            pltpu.VMEM((NZ, TOK, NEAR), BF16),
            pltpu.VMEM((TOK, FF), BF16),
            pltpu.VMEM((N_SP, CAP, D), BF16),
            pltpu.VMEM((N_SP, CAP, D), BF16),
            pltpu.VMEM((NZ // 2, NX, PLANE, 2, CAP, QUARTER), BF16),
            pltpu.VMEM((NZ // 2, NX * PLANE, 2, CAP, QUARTER), BF16),
            pltpu.VMEM((14, TOK, QUARTER // 2), BF16),
            pltpu.VMEM((14, TOK, QUARTER // 2), BF16),
            pltpu.VMEM((NZ, 8, TOK), F32),
            dma((14,)),
            dma((3,)),
            dma((4,)),
            dma((5,)),
            dma((4,)),
            dma((4,)),
            dma,
            dma,
            dma,
            dma((NZ,)),
            dma,
            dma((NZ,)),
            dma,
            dma,
            dma,
            dma((14,)),
            dma,
            dma,
        ],
        compiler_params=pltpu.CompilerParams(
            collective_id=0, has_side_effects=True, vmem_limit_bytes=60 << 20
        ),
        name="layer",
    )(
        memory_queries.T,
        memory_keys.T,
        memory_values.T,
        output_gate_preactivation.T,
        log_input_gate,
        forget_preactivation,
        head_forget_bias,
        forget_extra_boost,
        head_norm_gain.reshape(1, HW),
        memory_output_weight,
        residual,
        expert_norm_gain.reshape(1, D),
        routes.T,
        router_weight_matrix.T,
        routed_gate_weight,
        routed_up_weight,
        routed_down_weight,
        shared_gate_weight,
        shared_up_weight,
        shared_down_weight,
    )


def solution(mesh):
    split = Mesh(
        mesh.devices.reshape(NZ, NY, NC, mesh.shape["tp"]), ("sp_0", "sp_1", "sp_2", "tp")
    )
    return jax.shard_map(
        body,
        mesh=split,
        in_specs=(
            P(SP, "tp"),
            P(SP, "tp"),
            P(SP, "tp"),
            P(SP, "tp"),
            P("tp", SP),
            P("tp", SP),
            P("tp"),
            P("tp", SP),
            P("tp"),
            P(),
            P(SP, None),
            P(),
            P(SP, None),
            P(SP, None),
            P(SP, None, "tp"),
            P(SP, None, "tp"),
            P(SP, "tp", None),
            P(None, "tp"),
            P(None, "tp"),
            P("tp", None),
        ),
        out_specs=P(SP, "tp"),
        check_vma=False,
    )
```

```python
import jax
import jax.numpy as jnp
from jax import lax
from jax.experimental import pallas as pl
from jax.experimental.pallas import tpu as pltpu
from jax.sharding import Mesh
from jax.sharding import PartitionSpec as P

SP = ("sp_0", "sp_1", "sp_2")
MESH_ID = pl.DeviceIdType.MESH
NEG_LARGE = -1e30
EPSILON = 1e-06
F32 = jnp.float32
BF16 = jnp.bfloat16
HIGHEST = lax.Precision.HIGHEST

NZ, NY, NC, NX = 8, 4, 2, 4
PLANE = NY * NC
N_SP = NZ * PLANE
TOK = 256
DH = 96
HW = 192
D = 2048
FF = 512
GROUP = FF // NX
PART = GROUP // PLANE
CAP = 8
SLOTS = N_SP * CAP
NEAR = PLANE * NX * CAP
LANES = 128
SOON = 1280
SLICE = HW // PLANE
QUARTER = D // NX
CHUNK = 2 * PLANE


def nt(a, b, precision=None):
    return lax.dot_general(
        a, b, (((1,), (1,)), ((), ())), preferred_element_type=F32, precision=precision
    )


def tn(a, b, precision=None):
    return lax.dot_general(
        a, b, (((0,), (0,)), ((), ())), preferred_element_type=F32, precision=precision
    )


def nn(a, b, precision=None):
    return jnp.dot(a, b, preferred_element_type=F32, precision=precision)


def arrival(ref, sem):
    pltpu.make_async_copy(ref, ref, sem).wait()


def z_offset(i):
    return jnp.where(lax.rem(i, 2) == 0, 4 + i // 2, 4 - (i + 1) // 2)


def kernel(
    q_hbm,
    k_hbm,
    v_hbm,
    og_hbm,
    lig_hbm,
    fpre_hbm,
    bias_ref,
    boost_hbm,
    hgain_ref,
    wo_hbm,
    res_hbm,
    egain_ref,
    routes_hbm,
    rw_hbm,
    gate_hbm,
    up_hbm,
    down_hbm,
    sg_hbm,
    su_hbm,
    sd_hbm,
    out_ref,
    q_ref,
    k_ref,
    v_ref,
    og_ref,
    lig_ref,
    fpre_ref,
    boost_ref,
    wo_ref,
    res_ref,
    routes_ref,
    rw_ref,
    sg_ref,
    su_ref,
    sd_ref,
    wg_ref,
    wu_ref,
    wd_ref,
    state_ref,
    plane_ref,
    zst_ref,
    fin_ref,
    carry_ref,
    mix_ref,
    mixed_ref,
    hidden_ref,
    stream_ref,
    normed_ref,
    pick_ref,
    whi_ref,
    wlo_ref,
    shared_ref,
    sbuf_ref,
    rbuf_ref,
    eo_ref,
    near_ref,
    chain_out_ref,
    chain_in_ref,
    table_ref,
    in_sem,
    own_sem,
    wsend_sem,
    wrecv_sem,
    st_send,
    st_recv,
    mix_send,
    mix_recv,
    d_send,
    d_recv,
    b_send,
    b_recv,
    rs_ssem,
    rs_rsem,
    chain_send,
    chain_recv,
    swap_send,
    swap_recv,
):
    z, y, c, x = (lax.axis_index(a) for a in ("sp_0", "sp_1", "sp_2", "tp"))
    p = y * NC + c
    sp = z * PLANE + p

    def sp_dev(tz, tp_):
        return {"sp_0": tz, "sp_1": tp_ // NC, "sp_2": lax.rem(tp_, NC)}

    own_rows = pl.ds(pl.multiple_of(x * GROUP, GROUP), GROUP)

    def quarter_of(n):
        return pl.ds(pl.multiple_of(n * QUARTER, QUARTER), QUARTER)

    early = (
        (lig_hbm, lig_ref),
        (fpre_hbm, fpre_ref),
        (boost_hbm, boost_ref),
        (k_hbm, k_ref),
        (v_hbm, v_ref),
        (q_hbm, q_ref),
        (og_hbm, og_ref),
        (routes_hbm, routes_ref),
        (rw_hbm, rw_ref),
        (wo_hbm, wo_ref),
        (res_hbm, res_ref),
        (sg_hbm, sg_ref),
        (su_hbm, su_ref),
        (sd_hbm.at[:, quarter_of(x)], sd_ref.at[own_rows]),
    )
    loads = [pltpu.make_async_copy(a, b, in_sem.at[n]) for n, (a, b) in enumerate(early)]
    for cp in loads:
        cp.start()

    barrier = pltpu.get_barrier_semaphore()

    @pl.loop(1, NZ)
    def _(n):
        pl.semaphore_signal(
            barrier, inc=1, device_id={"sp_0": lax.rem(z + n, NZ)}, device_id_type=MESH_ID
        )

    @pl.loop(1, PLANE)
    def _(n):
        pl.semaphore_signal(
            barrier, inc=1, device_id=sp_dev(z, lax.rem(p + n, PLANE)), device_id_type=MESH_ID
        )

    for n in range(1, NX):
        pl.semaphore_signal(
            barrier, inc=1, device_id={"tp": lax.rem(x + n, NX)}, device_id_type=MESH_ID
        )

    own_weights = (
        pltpu.make_async_copy(
            gate_hbm.at[x], wg_ref.at[:, own_rows], own_sem.at[0]
        ),
        pltpu.make_async_copy(
            up_hbm.at[x], wu_ref.at[:, own_rows], own_sem.at[1]
        ),
        pltpu.make_async_copy(
            down_hbm.at[x], wd_ref.at[own_rows], own_sem.at[2]
        ),
    )

    for n in range(3):
        loads[n].wait()
    second = lax.broadcasted_iota(jnp.int32, (2, TOK), 0) == 1
    bias = jnp.where(second, bias_ref[1], bias_ref[0])
    pre = fpre_ref[...] + bias
    log_forget = jnp.minimum(pre, 0.0) - jnp.log1p(jnp.exp(-jnp.abs(pre))) + boost_ref[...]
    row = lax.broadcasted_iota(jnp.int32, (TOK, TOK), 0)
    col = lax.broadcasted_iota(jnp.int32, (TOK, TOK), 1)
    causal = row <= col
    upper = jnp.where(causal, 1.0, 0.0).astype(F32)
    eye = jnp.where(row == col, 1.0, 0.0).astype(F32)
    log_in = lig_ref[...]
    cumul = nn(log_forget, upper, HIGHEST)
    source = nt(eye, log_in - cumul, HIGHEST)
    ending = jnp.sum(log_forget, axis=1, keepdims=True)
    w_log = ending - cumul + log_in
    local_top = jnp.max(w_log, axis=1, keepdims=True)
    w_end = jnp.exp(w_log - local_top)

    loads[3].wait()
    loads[4].wait()
    lane = lax.broadcasted_iota(jnp.int32, (DH, LANES), 1)
    slice_lane = lax.broadcasted_iota(jnp.int32, (SLICE, LANES), 1)

    def with_scalars(mem, top, total, lanes):
        return jnp.where(lanes == DH, top, jnp.where(lanes == DH + 1, total, mem))

    def taken_apart(block):
        return block, block[:, DH : DH + 1], block[:, DH + 1 : DH + 2]

    padding = jnp.zeros((LANES - DH, TOK), F32)
    for h in range(2):
        keys = k_ref[h * DH : (h + 1) * DH].astype(F32) * w_end[h : h + 1]
        values = v_ref[h * DH : (h + 1) * DH].astype(F32)
        memory = nt(values, jnp.concatenate([keys, padding], axis=0), HIGHEST)
        state = with_scalars(memory, local_top[h : h + 1], ending[h : h + 1], lane)
        state_ref[h * (PLANE // 2) : (h + 1) * (PLANE // 2)] = state.reshape(PLANE // 2, SLICE, LANES)

    pl.semaphore_wait(barrier, NZ - 1 + PLANE - 1 + NX - 1)

    @pl.loop(1, PLANE)
    def _(n):
        to = lax.rem(p + n, PLANE)
        pltpu.make_async_remote_copy(
            state_ref.at[to],
            plane_ref.at[p],
            st_send.at[0],
            st_recv.at[0],
            device_id=sp_dev(z, to),
            device_id_type=MESH_ID,
        ).start()

    def send_weights(n, src, dst):
        for step in (2, 1, 3):
            to = lax.rem(x + step, NX)
            pltpu.make_async_remote_copy(
                src(to),
                dst,
                wsend_sem.at[n],
                wrecv_sem.at[n],
                device_id={"tp": to},
                device_id_type=MESH_ID,
            ).start()

    upper_half, lower_half = pl.ds(0, SOON), pl.ds(SOON, D - SOON)
    def part_rows(k):
        return pl.ds(pl.multiple_of(k * GROUP + p * PART, PART), PART)

    send_weights(
        3,
        lambda to: sd_hbm.at[
            pl.ds(pl.multiple_of(p * PART, PART), PART),
            quarter_of(to),
        ],
        sd_ref.at[part_rows(x)],
    )
    send_weights(0, lambda to: gate_hbm.at[to, upper_half], wg_ref.at[upper_half, own_rows])
    for cp in own_weights:
        cp.start()
    plane_ref[p] = state_ref[p]

    loads[5].wait()
    scale = DH ** (-0.5)
    local_max, numer = [], []
    for h in range(2):
        head = slice(h * DH, (h + 1) * DH)
        d_log = jnp.where(causal, cumul[h : h + 1] + source[:, h : h + 1], NEG_LARGE)
        top = jnp.max(d_log, axis=0, keepdims=True)
        scores = tn(k_ref[head], q_ref[head]) * scale
        within = (scores * jnp.exp(d_log - top)).astype(BF16)
        numer.append(nn(v_ref[head], within))
        local_max.append(top)

    def join(earlier, later):
        mem_a, top_a, total_a = earlier
        mem_b, top_b, total_b = later
        top = jnp.maximum(total_b + top_a, top_b)
        mem = jnp.exp(total_b + top_a - top) * mem_a + jnp.exp(top_b - top) * mem_b
        return mem, top, total_a + total_b

    none = (
        jnp.zeros((SLICE, LANES), F32),
        jnp.full((SLICE, 1), NEG_LARGE, F32),
        jnp.zeros((SLICE, 1), F32),
    )
    arrival(plane_ref.at[pl.ds(0, PLANE - 1)], st_recv.at[0])
    whole, before = none, []
    for n in range(PLANE):
        before.append(whole)
        whole = join(whole, taken_apart(plane_ref[n]))
    zst_ref[z] = with_scalars(*whole, slice_lane)

    @pl.loop(1, NZ)
    def _(n):
        pltpu.make_async_remote_copy(
            zst_ref.at[z],
            zst_ref.at[z],
            st_send.at[1],
            st_recv.at[1],
            device_id={"sp_0": lax.rem(z + n, NZ)},
            device_id_type=MESH_ID,
        ).start()

    loads[7].wait()
    loads[8].wait()
    table_ref[z] = jnp.concatenate([routes_ref[...].astype(F32), rw_ref[...]], axis=0)

    @pl.loop(1, NZ)
    def _(n):
        pltpu.make_async_remote_copy(
            table_ref.at[z],
            table_ref.at[z],
            st_send.at[3],
            st_recv.at[3],
            device_id={"sp_0": lax.rem(z + n, NZ)},
            device_id_type=MESH_ID,
        ).start()

    slot = lax.broadcasted_iota(jnp.int32, (SLOTS, TOK), 0)
    expert = slot // CAP * NX + x
    named = jnp.zeros((SLOTS, TOK), F32)
    for n in range(4):
        named = jnp.where(routes_ref[n : n + 1] == expert, 1.0, named)
    strict = jnp.where(row < col, 1.0, 0.0).astype(BF16)
    rank = nn(named.astype(BF16), strict)
    pick_ref[...] = jnp.where(rank == lax.rem(slot, CAP).astype(F32), named, 0.0).astype(BF16)
    hgain = nt(eye[:HW, :HW], hgain_ref[...], HIGHEST)
    loads[6].wait()
    gating = hgain * jax.nn.sigmoid(og_ref[...].astype(F32))

    arrival(zst_ref.at[pl.ds(0, NZ - 1)], st_recv.at[1])
    carried = none
    for n in range(NZ):
        mem, top, total = taken_apart(zst_ref[n])
        passed = n < z
        carried = join(
            carried, (mem, jnp.where(passed, top, NEG_LARGE), jnp.where(passed, total, 0.0))
        )
    z_mem, z_top, z_total = carried
    z_mem = jnp.where(z > 0, z_mem, 0.0)
    for n in range(PLANE):
        fin_ref[n] = with_scalars(*join((z_mem, z_top, z_total), before[n]), slice_lane)

    @pl.loop(1, PLANE)
    def _(n):
        to = lax.rem(p + n, PLANE)
        pltpu.make_async_remote_copy(
            fin_ref.at[to],
            carry_ref.at[p],
            st_send.at[2],
            st_recv.at[2],
            device_id=sp_dev(z, to),
            device_id_type=MESH_ID,
        ).start()

    carry_ref[p] = fin_ref[p]
    arrival(carry_ref.at[pl.ds(0, PLANE - 1)], st_recv.at[2])
    no_queries = jnp.zeros((LANES - DH, TOK), BF16)
    for h in range(2):
        head = slice(h * DH, (h + 1) * DH)
        memory = carry_ref[h * (PLANE // 2) : (h + 1) * (PLANE // 2)].reshape(DH, LANES)
        carry_top = memory[0:1, DH : DH + 1]
        memory = jnp.where(lane < DH, memory, 0.0)
        high = memory.astype(BF16)
        low = (memory - high.astype(F32)).astype(BF16)
        queries = jnp.concatenate([q_ref[head], no_queries], axis=0)
        inter = nn(high, queries) + nn(low, queries)
        g_log = cumul[h : h + 1] + carry_top
        stab = jnp.maximum(g_log, local_max[h])
        cell = numer[h] * jnp.exp(local_max[h] - stab) + inter * (jnp.exp(g_log - stab) * scale)
        mean = jnp.sum(cell * cell, axis=0, keepdims=True) / DH
        mix_ref[x, head] = (cell * lax.rsqrt(mean + EPSILON) * gating[head]).astype(BF16)
    for step in (1, 3, 2):
        pltpu.make_async_remote_copy(
            mix_ref.at[x],
            mix_ref.at[x],
            mix_send,
            mix_recv.at[step % 2],
            device_id={"tp": lax.rem(x + step, NX)},
            device_id_type=MESH_ID,
        ).start()
    send_weights(0, lambda to: gate_hbm.at[to, lower_half], wg_ref.at[lower_half, own_rows])
    send_weights(1, lambda to: up_hbm.at[to], wu_ref.at[:, own_rows])
    for j in (0, 1, 3, 2):
        for step in (2, 1, 3):
            to = lax.rem(x + step, NX)
            columns = quarter_of(lax.rem(to + j, NX))
            pltpu.make_async_remote_copy(
                down_hbm.at[to, :, columns],
                wd_ref.at[own_rows, columns],
                wsend_sem.at[2],
                wrecv_sem.at[4 if j == 2 else 2],
                device_id={"tp": to},
                device_id_type=MESH_ID,
            ).start()

    loads[9].wait()
    loads[10].wait()

    def turned(k):
        return jnp.transpose(mix_ref[lax.rem(x + k, NX)].astype(F32)).astype(BF16)

    mixed_ref[0] = turned(0)
    arrival(mix_ref.at[pl.ds(0, 2)], mix_recv.at[1])
    mixed_ref[1] = turned(1)
    mixed_ref[2] = turned(3)

    @pl.loop(0, NX)
    def _(n):
        columns = quarter_of(n)
        part = res_ref[:, columns].astype(F32)
        for m, k in enumerate((0, 1, 3)):
            part = part + nn(mixed_ref[m], wo_ref[lax.rem(x + k, NX), :, columns])
        stream_ref[n] = part

    arrival(mix_ref.at[0], mix_recv.at[0])
    mixed_ref[3] = turned(2)

    def project(n, total):
        part = stream_ref[n] + nn(mixed_ref[3], wo_ref[lax.rem(x + 2, NX), :, quarter_of(n)])
        stream_ref[n] = part
        return total + jnp.sum(part * part, axis=1, keepdims=True)

    square = lax.fori_loop(0, NX, project, jnp.zeros((TOK, 1), F32))
    inverse = lax.rsqrt(square / D + EPSILON)

    @pl.loop(0, NX)
    def _(n):
        columns = quarter_of(n)
        normed_ref[:, columns] = (stream_ref[n] * inverse * egain_ref[:, columns]).astype(BF16)

    @pl.loop(0, NZ)
    def _(i):
        to_z = lax.rem(z + z_offset(i), NZ)
        chosen = pick_ref[pl.ds(pl.multiple_of(to_z * PLANE * CAP, PLANE * CAP), PLANE * CAP)]
        rows = nn(chosen, normed_ref[...])
        sbuf_ref[pl.ds(i * PLANE, PLANE)] = rows.reshape(PLANE, CAP, D).astype(BF16)

        @pl.loop(0, PLANE)
        def _(n):
            to = lax.rem(p + n, PLANE)
            itself = (i == NZ - 1) & (n == 0)

            @pl.when(jnp.logical_not(itself))
            def _():
                pltpu.make_async_remote_copy(
                    sbuf_ref.at[i * PLANE + to],
                    rbuf_ref.at[i * PLANE + p],
                    d_send,
                    d_recv.at[i],
                    device_id=sp_dev(to_z, to),
                    device_id_type=MESH_ID,
                ).start()

            @pl.when(itself)
            def _():
                pltpu.make_async_copy(
                    sbuf_ref.at[i * PLANE + to], rbuf_ref.at[i * PLANE + p], d_recv.at[i]
                ).start()

    arrival(sd_ref.at[pl.ds(0, (NX - 1) * PART)], wrecv_sem.at[3])
    for step in range(1, NX):
        rows = part_rows(lax.rem(x + step, NX))

        @pl.loop(1, PLANE)
        def _(n):
            pltpu.make_async_remote_copy(
                sd_ref.at[rows],
                sd_ref.at[rows],
                swap_send,
                swap_recv,
                device_id=sp_dev(z, lax.rem(p + n, PLANE)),
                device_id_type=MESH_ID,
            ).start()

    for n in range(11, 14):
        loads[n].wait()
    normed = normed_ref[...]
    shared_hidden = jax.nn.silu(nn(normed, sg_ref[...])) * nn(normed, su_ref[...])
    shared_ref[:, own_rows] = shared_hidden.astype(BF16)

    arrival(table_ref.at[pl.ds(0, NZ - 1)], st_recv.at[3])
    slot = lax.broadcasted_iota(jnp.int32, (NEAR, TOK), 0)
    expert = (slot // CAP + z * (PLANE * NX)).astype(F32)
    place = lax.rem(slot, CAP).astype(F32)

    @pl.loop(0, NZ)
    def _(n):
        table = table_ref[n]
        named = jnp.zeros((NEAR, TOK), F32)
        weight = jnp.zeros((NEAR, TOK), F32)
        for k in range(4):
            hit = table[k : k + 1] == expert
            named = jnp.where(hit, 1.0, named)
            weight = jnp.where(hit, table[k + 4 : k + 5], weight)
        rank = nn(named.astype(BF16), strict)
        weight = jnp.transpose(jnp.where(rank == place, weight, 0.0))
        high = weight.astype(BF16)
        whi_ref[n] = high
        wlo_ref[n] = (weight - high.astype(F32)).astype(BF16)

    for cp in own_weights:
        cp.wait()
    arrival(wg_ref.at[:, pl.ds(0, FF - GROUP)], wrecv_sem.at[0])
    arrival(wu_ref.at[:, pl.ds(0, FF - GROUP)], wrecv_sem.at[1])

    @pl.loop(0, NZ // 2)
    def _(s):
        arrival(rbuf_ref.at[pl.ds(0, PLANE)], d_recv.at[2 * s])
        arrival(rbuf_ref.at[pl.ds(0, PLANE)], d_recv.at[2 * s + 1])
        blocks = pl.ds(pl.multiple_of(s * CHUNK, CHUNK), CHUNK)
        rows = rbuf_ref[blocks].astype(F32).reshape(CHUNK * CAP, D).astype(BF16)
        hidden = jax.nn.silu(nn(rows, wg_ref[...])) * nn(rows, wu_ref[...])
        hidden_ref[s] = hidden.astype(BF16)

    arrival(wd_ref.at[pl.ds(0, FF - GROUP), pl.ds(0, D - QUARTER)], wrecv_sem.at[2])

    def send_back(src, dst, sem, columns):
        for j in columns:
            to_x = lax.rem(x + j, NX)

            @pl.loop(0 if j else 1, PLANE)
            def _(n):
                to = lax.rem(p + n, PLANE)
                pltpu.make_async_remote_copy(
                    src(to_x, to),
                    dst,
                    b_send,
                    sem,
                    device_id={**sp_dev(z, to), "tp": to_x},
                    device_id_type=MESH_ID,
                ).start()

            if j == 0:
                pltpu.make_async_copy(src(x, p), dst, sem).start()

    def out_of_expert(s, k, rows, columns):
        for j in columns:
            n = lax.rem(x + j, NX)
            result = nn(rows, wd_ref[:, quarter_of(n)])
            result = result.reshape(-1, PLANE, CAP, QUARTER).astype(BF16)
            for m in range(result.shape[0]):
                eo_ref[s, n, :, k + m] = result[m]

    def one_back(i, columns):
        s, k = i // 2, i % 2
        rows = hidden_ref[s, k * (PLANE * CAP) : (k + 1) * (PLANE * CAP)]
        out_of_expert(s, k, rows, columns)
        send_back(
            lambda to_x, to: eo_ref.at[s, to_x, to, k],
            near_ref.at[s, p * NX + x, k],
            b_recv.at[i],
            columns,
        )

    width = QUARTER // 2

    def weighted(i, h):
        block = lax.rem(z + NZ - z_offset(i), NZ)
        rows = near_ref[i // 2, :, i % 2, :, h * width : (h + 1) * width]
        rows = rows.astype(F32).reshape(NEAR, width).astype(BF16)
        return nn(whi_ref[block], rows) + nn(wlo_ref[block], rows)

    def arrived(i, h):
        arrival(chain_in_ref.at[2 * i + h], chain_recv.at[2 * i + h])
        return chain_in_ref[2 * i + h].astype(F32)

    def passed_on(i, h, before, up):
        part = weighted(i, h)
        if before is not None:
            part = part + arrived(before, h)
        chain_out_ref[2 * i + h] = part.astype(BF16)
        pltpu.make_async_remote_copy(
            chain_out_ref.at[2 * i + h],
            chain_in_ref.at[2 * i + h],
            chain_send,
            chain_recv.at[2 * i + h],
            device_id={"sp_0": lax.rem(z + (1 if up else NZ - 1), NZ)},
            device_id_type=MESH_ID,
        ).start()

    soon, every = (1, 3, 0), (2, 1, 3, 0)

    def returned(i):
        arrival(near_ref.at[i // 2, :, i % 2], b_recv.at[i])

    one_back(0, soon)
    arrival(wd_ref.at[pl.ds(0, FF - GROUP), pl.ds(0, QUARTER)], wrecv_sem.at[4])
    one_back(0, (2,))
    one_back(1, every)
    one_back(2, every)
    one_back(3, every)
    returned(0)
    passed_on(0, 0, None, True)
    passed_on(0, 1, None, False)
    one_back(4, every)
    returned(1)
    passed_on(1, 0, None, False)
    one_back(5, every)
    returned(2)
    passed_on(2, 1, None, True)
    passed_on(2, 0, 0, True)
    passed_on(1, 1, 0, False)
    one_back(6, every)
    returned(3)
    passed_on(3, 0, 1, False)
    one_back(7, every)
    for step in (2, 1, 3):
        pltpu.make_async_remote_copy(
            shared_ref.at[:, own_rows],
            shared_ref.at[:, own_rows],
            rs_ssem,
            rs_rsem,
            device_id={"tp": lax.rem(x + step, NX)},
            device_id_type=MESH_ID,
        ).start()
    returned(4)
    passed_on(4, 1, 2, True)
    passed_on(3, 1, 1, False)
    passed_on(4, 0, 2, True)
    returned(5)
    passed_on(5, 0, 3, False)
    returned(6)
    passed_on(6, 1, 4, True)
    passed_on(5, 1, 3, False)
    passed_on(6, 0, 4, True)

    arrival(near_ref.at[3, :, 1], b_recv.at[7])
    totals = []
    for h in range(2):
        totals.append(stream_ref[x, :, h * width : (h + 1) * width] + weighted(NZ - 1, h))
    arrival(sd_ref.at[pl.ds(0, (NX - 1) * (GROUP - PART))], swap_recv)
    arrival(shared_ref.at[:, pl.ds(0, FF - GROUP)], rs_rsem)
    for h in range(2):
        columns = slice(h * width, (h + 1) * width)
        total = totals[h] + nn(shared_ref[...], sd_ref[:, columns])
        total = total + arrived(5, h) + arrived(6, h)
        out_ref[:, columns] = total.astype(BF16)

    arrival(plane_ref.at[pl.ds(0, PLANE - 1)], st_send.at[0])
    arrival(zst_ref.at[pl.ds(0, NZ - 1)], st_send.at[1])
    arrival(fin_ref.at[pl.ds(0, PLANE - 1)], st_send.at[2])
    arrival(mix_ref.at[pl.ds(0, NX - 1)], mix_send)
    arrival(wg_ref.at[:, pl.ds(0, FF - GROUP)], wsend_sem.at[0])
    arrival(wu_ref.at[:, pl.ds(0, FF - GROUP)], wsend_sem.at[1])
    arrival(wd_ref.at[pl.ds(0, FF - GROUP)], wsend_sem.at[2])
    arrival(sbuf_ref.at[pl.ds(0, N_SP - 1)], d_send)
    arrival(table_ref.at[pl.ds(0, NZ - 1)], st_send.at[3])
    for n in range(NZ // 2):
        arrival(near_ref.at[n, pl.ds(0, NX * PLANE - 1)], b_send)
    arrival(sd_ref.at[pl.ds(0, (NX - 1) * PART)], wsend_sem.at[3])
    arrival(sd_ref.at[pl.ds(0, (NX - 1) * (GROUP - PART))], swap_send)
    arrival(shared_ref.at[:, pl.ds(0, FF - GROUP)], rs_ssem)
    arrival(chain_out_ref, chain_send)


def body(
    memory_queries,
    memory_keys,
    memory_values,
    output_gate_preactivation,
    log_input_gate,
    forget_preactivation,
    head_forget_bias,
    forget_extra_boost,
    head_norm_gain,
    memory_output_weight,
    residual,
    expert_norm_gain,
    routes,
    router_weight_matrix,
    routed_gate_weight,
    routed_up_weight,
    routed_down_weight,
    shared_gate_weight,
    shared_up_weight,
    shared_down_weight,
):
    anywhere = pl.BlockSpec(memory_space=pl.ANY)
    vmem = pl.BlockSpec(memory_space=pltpu.VMEM)
    smem = pl.BlockSpec(memory_space=pltpu.SMEM)
    specs = [anywhere] * 20
    specs[6] = smem
    specs[8] = vmem
    specs[11] = vmem
    dma = pltpu.SemaphoreType.DMA
    return pl.pallas_call(
        kernel,
        out_shape=jax.ShapeDtypeStruct((TOK, QUARTER), BF16),
        in_specs=specs,
        out_specs=vmem,
        scratch_shapes=[
            pltpu.VMEM((HW, TOK), BF16),
            pltpu.VMEM((HW, TOK), BF16),
            pltpu.VMEM((HW, TOK), BF16),
            pltpu.VMEM((HW, TOK), BF16),
            pltpu.VMEM((2, TOK), F32),
            pltpu.VMEM((2, TOK), F32),
            pltpu.VMEM((2, TOK), F32),
            pltpu.VMEM((NX, HW, D), BF16),
            pltpu.VMEM((TOK, D), BF16),
            pltpu.VMEM((4, TOK), jnp.int32),
            pltpu.VMEM((4, TOK), F32),
            pltpu.VMEM((D, GROUP), BF16),
            pltpu.VMEM((D, GROUP), BF16),
            pltpu.VMEM((FF, QUARTER), BF16),
            pltpu.VMEM((D, FF), BF16),
            pltpu.VMEM((D, FF), BF16),
            pltpu.VMEM((FF, D), BF16),
            pltpu.VMEM((PLANE, SLICE, LANES), F32),
            pltpu.VMEM((PLANE, SLICE, LANES), F32),
            pltpu.VMEM((NZ, SLICE, LANES), F32),
            pltpu.VMEM((PLANE, SLICE, LANES), F32),
            pltpu.VMEM((PLANE, SLICE, LANES), F32),
            pltpu.VMEM((NX, HW, TOK), BF16),
            pltpu.VMEM((NX, TOK, HW), BF16),
            pltpu.VMEM((NZ // 2, CHUNK * CAP, FF), BF16),
            pltpu.VMEM((NX, TOK, QUARTER), F32),
            pltpu.VMEM((TOK, D), BF16),
            pltpu.VMEM((SLOTS, TOK), BF16),
            pltpu.VMEM((NZ, TOK, NEAR), BF16),
            pltpu.VMEM((NZ, TOK, NEAR), BF16),
            pltpu.VMEM((TOK, FF), BF16),
            pltpu.VMEM((N_SP, CAP, D), BF16),
            pltpu.VMEM((N_SP, CAP, D), BF16),
            pltpu.VMEM((NZ // 2, NX, PLANE, 2, CAP, QUARTER), BF16),
            pltpu.VMEM((NZ // 2, NX * PLANE, 2, CAP, QUARTER), BF16),
            pltpu.VMEM((14, TOK, QUARTER // 2), BF16),
            pltpu.VMEM((14, TOK, QUARTER // 2), BF16),
            pltpu.VMEM((NZ, 8, TOK), F32),
            dma((14,)),
            dma((3,)),
            dma((4,)),
            dma((5,)),
            dma((4,)),
            dma((4,)),
            dma,
            dma((2,)),
            dma,
            dma((NZ,)),
            dma,
            dma((NZ,)),
            dma,
            dma,
            dma,
            dma((14,)),
            dma,
            dma,
        ],
        compiler_params=pltpu.CompilerParams(
            collective_id=0, has_side_effects=True, vmem_limit_bytes=60 << 20
        ),
        name="layer",
    )(
        memory_queries.T,
        memory_keys.T,
        memory_values.T,
        output_gate_preactivation.T,
        log_input_gate,
        forget_preactivation,
        head_forget_bias,
        forget_extra_boost,
        head_norm_gain.reshape(1, HW),
        memory_output_weight.reshape(NX, HW, D),
        residual,
        expert_norm_gain.reshape(1, D),
        routes.T,
        router_weight_matrix.T,
        routed_gate_weight,
        routed_up_weight,
        routed_down_weight,
        shared_gate_weight,
        shared_up_weight,
        shared_down_weight,
    )


def solution(mesh):
    split = Mesh(
        mesh.devices.reshape(NZ, NY, NC, mesh.shape["tp"]), ("sp_0", "sp_1", "sp_2", "tp")
    )
    return jax.shard_map(
        body,
        mesh=split,
        in_specs=(
            P(SP, "tp"),
            P(SP, "tp"),
            P(SP, "tp"),
            P(SP, "tp"),
            P("tp", SP),
            P("tp", SP),
            P("tp"),
            P("tp", SP),
            P("tp"),
            P(),
            P(SP, None),
            P(),
            P(SP, None),
            P(SP, None),
            P(SP, None, "tp"),
            P(SP, None, "tp"),
            P(SP, "tp", None),
            P(None, "tp"),
            P(None, "tp"),
            P("tp", None),
        ),
        out_specs=P(SP, "tp"),
        check_vma=False,
    )
```

```python
import jax
import jax.numpy as jnp
from jax import lax
from jax.experimental import pallas as pl
from jax.experimental.pallas import tpu as pltpu
from jax.sharding import Mesh
from jax.sharding import PartitionSpec as P

SP = ("sp_0", "sp_1", "sp_2")
MESH_ID = pl.DeviceIdType.MESH
NEG_LARGE = -1e30
EPSILON = 1e-06
F32 = jnp.float32
BF16 = jnp.bfloat16
HIGHEST = lax.Precision.HIGHEST

NZ, NY, NC, NX = 8, 4, 2, 4
PLANE = NY * NC
N_SP = NZ * PLANE
TOK = 256
DH = 96
HW = 192
D = 2048
FF = 512
GROUP = FF // NX
PART = GROUP // PLANE
CAP = 8
SLOTS = N_SP * CAP
NEAR = PLANE * NX * CAP
LANES = 128
SOON = 1280
SLICE = HW // PLANE
QUARTER = D // NX
CHUNK = 2 * PLANE


def nt(a, b, precision=None):
    return lax.dot_general(
        a, b, (((1,), (1,)), ((), ())), preferred_element_type=F32, precision=precision
    )


def tn(a, b, precision=None):
    return lax.dot_general(
        a, b, (((0,), (0,)), ((), ())), preferred_element_type=F32, precision=precision
    )


def nn(a, b, precision=None):
    return jnp.dot(a, b, preferred_element_type=F32, precision=precision)


def arrival(ref, sem):
    pltpu.make_async_copy(ref, ref, sem).wait()


def z_offset(i):
    return jnp.where(lax.rem(i, 2) == 0, 4 + i // 2, 4 - (i + 1) // 2)


def kernel(
    q_hbm,
    k_hbm,
    v_hbm,
    og_hbm,
    lig_hbm,
    fpre_hbm,
    bias_ref,
    boost_hbm,
    hgain_ref,
    wo_hbm,
    res_hbm,
    egain_ref,
    routes_hbm,
    rw_hbm,
    gate_hbm,
    up_hbm,
    down_hbm,
    sg_hbm,
    su_hbm,
    sd_hbm,
    out_ref,
    q_ref,
    k_ref,
    v_ref,
    og_ref,
    lig_ref,
    fpre_ref,
    boost_ref,
    wo_ref,
    res_ref,
    routes_ref,
    rw_ref,
    sg_ref,
    su_ref,
    sd_ref,
    wg_ref,
    wu_ref,
    wd_ref,
    state_ref,
    plane_ref,
    zst_ref,
    fin_ref,
    carry_ref,
    mix_ref,
    mixed_ref,
    hidden_ref,
    stream_ref,
    normed_ref,
    pick_ref,
    whi_ref,
    wlo_ref,
    shared_ref,
    sbuf_ref,
    rbuf_ref,
    eo_ref,
    near_ref,
    chain_out_ref,
    chain_in_ref,
    table_ref,
    in_sem,
    own_sem,
    wsend_sem,
    wrecv_sem,
    st_send,
    st_recv,
    mix_send,
    mix_recv,
    d_send,
    d_recv,
    b_send,
    b_recv,
    rs_ssem,
    rs_rsem,
    chain_send,
    chain_recv,
    swap_send,
    swap_recv,
):
    z, y, c, x = (lax.axis_index(a) for a in ("sp_0", "sp_1", "sp_2", "tp"))
    p = y * NC + c
    sp = z * PLANE + p

    def sp_dev(tz, tp_):
        return {"sp_0": tz, "sp_1": tp_ // NC, "sp_2": lax.rem(tp_, NC)}

    own_rows = pl.ds(pl.multiple_of(x * GROUP, GROUP), GROUP)

    def quarter_of(n):
        return pl.ds(pl.multiple_of(n * QUARTER, QUARTER), QUARTER)

    early = (
        (lig_hbm, lig_ref),
        (fpre_hbm, fpre_ref),
        (boost_hbm, boost_ref),
        (k_hbm, k_ref),
        (v_hbm, v_ref),
        (q_hbm, q_ref),
        (og_hbm, og_ref),
        (routes_hbm, routes_ref),
        (rw_hbm, rw_ref),
        (wo_hbm, wo_ref),
        (res_hbm, res_ref),
        (sg_hbm, sg_ref),
        (su_hbm, su_ref),
        (sd_hbm.at[:, quarter_of(x)], sd_ref.at[own_rows]),
    )
    loads = [pltpu.make_async_copy(a, b, in_sem.at[n]) for n, (a, b) in enumerate(early)]
    for cp in loads:
        cp.start()

    barrier = pltpu.get_barrier_semaphore()

    @pl.loop(1, NZ)
    def _(n):
        pl.semaphore_signal(
            barrier, inc=1, device_id={"sp_0": lax.rem(z + n, NZ)}, device_id_type=MESH_ID
        )

    @pl.loop(1, PLANE)
    def _(n):
        pl.semaphore_signal(
            barrier, inc=1, device_id=sp_dev(z, lax.rem(p + n, PLANE)), device_id_type=MESH_ID
        )

    for n in range(1, NX):
        pl.semaphore_signal(
            barrier, inc=1, device_id={"tp": lax.rem(x + n, NX)}, device_id_type=MESH_ID
        )

    own_weights = (
        pltpu.make_async_copy(
            gate_hbm.at[x], wg_ref.at[:, own_rows], own_sem.at[0]
        ),
        pltpu.make_async_copy(
            up_hbm.at[x], wu_ref.at[:, own_rows], own_sem.at[1]
        ),
        pltpu.make_async_copy(
            down_hbm.at[x], wd_ref.at[own_rows], own_sem.at[2]
        ),
    )

    for n in range(3):
        loads[n].wait()
    second = lax.broadcasted_iota(jnp.int32, (2, TOK), 0) == 1
    bias = jnp.where(second, bias_ref[1], bias_ref[0])
    pre = fpre_ref[...] + bias
    log_forget = jnp.minimum(pre, 0.0) - jnp.log1p(jnp.exp(-jnp.abs(pre))) + boost_ref[...]
    row = lax.broadcasted_iota(jnp.int32, (TOK, TOK), 0)
    col = lax.broadcasted_iota(jnp.int32, (TOK, TOK), 1)
    causal = row <= col
    upper = jnp.where(causal, 1.0, 0.0).astype(F32)
    eye = jnp.where(row == col, 1.0, 0.0).astype(F32)
    log_in = lig_ref[...]
    cumul = nn(log_forget, upper, HIGHEST)
    source = nt(eye, log_in - cumul, HIGHEST)
    ending = jnp.sum(log_forget, axis=1, keepdims=True)
    w_log = ending - cumul + log_in
    local_top = jnp.max(w_log, axis=1, keepdims=True)
    w_end = jnp.exp(w_log - local_top)

    loads[3].wait()
    loads[4].wait()
    lane = lax.broadcasted_iota(jnp.int32, (DH, LANES), 1)
    slice_lane = lax.broadcasted_iota(jnp.int32, (SLICE, LANES), 1)

    def with_scalars(mem, top, total, lanes):
        return jnp.where(lanes == DH, top, jnp.where(lanes == DH + 1, total, mem))

    def taken_apart(block):
        return block, block[:, DH : DH + 1], block[:, DH + 1 : DH + 2]

    padding = jnp.zeros((LANES - DH, TOK), F32)
    for h in range(2):
        keys = k_ref[h * DH : (h + 1) * DH].astype(F32) * w_end[h : h + 1]
        values = v_ref[h * DH : (h + 1) * DH].astype(F32)
        memory = nt(values, jnp.concatenate([keys, padding], axis=0), HIGHEST)
        state = with_scalars(memory, local_top[h : h + 1], ending[h : h + 1], lane)
        state_ref[h * (PLANE // 2) : (h + 1) * (PLANE // 2)] = state.reshape(PLANE // 2, SLICE, LANES)

    pl.semaphore_wait(barrier, NZ - 1 + PLANE - 1 + NX - 1)

    @pl.loop(1, PLANE)
    def _(n):
        to = lax.rem(p + n, PLANE)
        pltpu.make_async_remote_copy(
            state_ref.at[to],
            plane_ref.at[p],
            st_send.at[0],
            st_recv.at[0],
            device_id=sp_dev(z, to),
            device_id_type=MESH_ID,
        ).start()

    def send_weights(n, src, dst):
        for step in (2, 1, 3):
            to = lax.rem(x + step, NX)
            pltpu.make_async_remote_copy(
                src(to),
                dst,
                wsend_sem.at[n],
                wrecv_sem.at[n],
                device_id={"tp": to},
                device_id_type=MESH_ID,
            ).start()

    upper_half, lower_half = pl.ds(0, SOON), pl.ds(SOON, D - SOON)
    def part_rows(k):
        return pl.ds(pl.multiple_of(k * GROUP + p * PART, PART), PART)

    send_weights(
        3,
        lambda to: sd_hbm.at[
            pl.ds(pl.multiple_of(p * PART, PART), PART),
            quarter_of(to),
        ],
        sd_ref.at[part_rows(x)],
    )
    send_weights(0, lambda to: gate_hbm.at[to, upper_half], wg_ref.at[upper_half, own_rows])
    for cp in own_weights:
        cp.start()
    plane_ref[p] = state_ref[p]

    loads[5].wait()
    scale = DH ** (-0.5)
    local_max, numer = [], []
    for h in range(2):
        head = slice(h * DH, (h + 1) * DH)
        d_log = jnp.where(causal, cumul[h : h + 1] + source[:, h : h + 1], NEG_LARGE)
        top = jnp.max(d_log, axis=0, keepdims=True)
        scores = tn(k_ref[head], q_ref[head]) * scale
        within = (scores * jnp.exp(d_log - top)).astype(BF16)
        numer.append(nn(v_ref[head], within))
        local_max.append(top)

    def join(earlier, later):
        mem_a, top_a, total_a = earlier
        mem_b, top_b, total_b = later
        top = jnp.maximum(total_b + top_a, top_b)
        mem = jnp.exp(total_b + top_a - top) * mem_a + jnp.exp(top_b - top) * mem_b
        return mem, top, total_a + total_b

    none = (
        jnp.zeros((SLICE, LANES), F32),
        jnp.full((SLICE, 1), NEG_LARGE, F32),
        jnp.zeros((SLICE, 1), F32),
    )
    arrival(plane_ref.at[pl.ds(0, PLANE - 1)], st_recv.at[0])
    whole, before = none, []
    for n in range(PLANE):
        before.append(whole)
        whole = join(whole, taken_apart(plane_ref[n]))
    zst_ref[z] = with_scalars(*whole, slice_lane)

    @pl.loop(1, NZ)
    def _(n):
        pltpu.make_async_remote_copy(
            zst_ref.at[z],
            zst_ref.at[z],
            st_send.at[1],
            st_recv.at[1],
            device_id={"sp_0": lax.rem(z + n, NZ)},
            device_id_type=MESH_ID,
        ).start()

    loads[7].wait()
    loads[8].wait()
    table_ref[z] = jnp.concatenate([routes_ref[...].astype(F32), rw_ref[...]], axis=0)

    @pl.loop(1, NZ)
    def _(n):
        pltpu.make_async_remote_copy(
            table_ref.at[z],
            table_ref.at[z],
            st_send.at[3],
            st_recv.at[3],
            device_id={"sp_0": lax.rem(z + n, NZ)},
            device_id_type=MESH_ID,
        ).start()

    slot = lax.broadcasted_iota(jnp.int32, (SLOTS, TOK), 0)
    expert = slot // CAP * NX + x
    named = jnp.zeros((SLOTS, TOK), F32)
    for n in range(4):
        named = jnp.where(routes_ref[n : n + 1] == expert, 1.0, named)
    strict = jnp.where(row < col, 1.0, 0.0).astype(BF16)
    rank = nn(named.astype(BF16), strict)
    pick_ref[...] = jnp.where(rank == lax.rem(slot, CAP).astype(F32), named, 0.0).astype(BF16)
    hgain = nt(eye[:HW, :HW], hgain_ref[...], HIGHEST)
    loads[6].wait()
    gating = hgain * jax.nn.sigmoid(og_ref[...].astype(F32))

    arrival(zst_ref.at[pl.ds(0, NZ - 1)], st_recv.at[1])
    carried = none
    for n in range(NZ):
        mem, top, total = taken_apart(zst_ref[n])
        passed = n < z
        carried = join(
            carried, (mem, jnp.where(passed, top, NEG_LARGE), jnp.where(passed, total, 0.0))
        )
    z_mem, z_top, z_total = carried
    z_mem = jnp.where(z > 0, z_mem, 0.0)
    for n in range(PLANE):
        fin_ref[n] = with_scalars(*join((z_mem, z_top, z_total), before[n]), slice_lane)

    @pl.loop(1, PLANE)
    def _(n):
        to = lax.rem(p + n, PLANE)
        pltpu.make_async_remote_copy(
            fin_ref.at[to],
            carry_ref.at[p],
            st_send.at[2],
            st_recv.at[2],
            device_id=sp_dev(z, to),
            device_id_type=MESH_ID,
        ).start()

    carry_ref[p] = fin_ref[p]
    arrival(carry_ref.at[pl.ds(0, PLANE - 1)], st_recv.at[2])
    no_queries = jnp.zeros((LANES - DH, TOK), BF16)
    for h in range(2):
        head = slice(h * DH, (h + 1) * DH)
        memory = carry_ref[h * (PLANE // 2) : (h + 1) * (PLANE // 2)].reshape(DH, LANES)
        carry_top = memory[0:1, DH : DH + 1]
        memory = jnp.where(lane < DH, memory, 0.0)
        high = memory.astype(BF16)
        low = (memory - high.astype(F32)).astype(BF16)
        queries = jnp.concatenate([q_ref[head], no_queries], axis=0)
        inter = nn(high, queries) + nn(low, queries)
        g_log = cumul[h : h + 1] + carry_top
        stab = jnp.maximum(g_log, local_max[h])
        cell = numer[h] * jnp.exp(local_max[h] - stab) + inter * (jnp.exp(g_log - stab) * scale)
        mean = jnp.sum(cell * cell, axis=0, keepdims=True) / DH
        mix_ref[x, head] = (cell * lax.rsqrt(mean + EPSILON) * gating[head]).astype(BF16)
    for step in (1, 3, 2):
        pltpu.make_async_remote_copy(
            mix_ref.at[x],
            mix_ref.at[x],
            mix_send,
            mix_recv.at[step % 2],
            device_id={"tp": lax.rem(x + step, NX)},
            device_id_type=MESH_ID,
        ).start()
    send_weights(0, lambda to: gate_hbm.at[to, lower_half], wg_ref.at[lower_half, own_rows])
    send_weights(1, lambda to: up_hbm.at[to], wu_ref.at[:, own_rows])
    for j in (0, 1, 3, 2):
        for step in (2, 1, 3):
            to = lax.rem(x + step, NX)
            columns = quarter_of(lax.rem(to + j, NX))
            pltpu.make_async_remote_copy(
                down_hbm.at[to, :, columns],
                wd_ref.at[own_rows, columns],
                wsend_sem.at[2],
                wrecv_sem.at[4 if j == 2 else 2],
                device_id={"tp": to},
                device_id_type=MESH_ID,
            ).start()

    loads[9].wait()
    loads[10].wait()

    def turned(k):
        return jnp.transpose(mix_ref[lax.rem(x + k, NX)].astype(F32)).astype(BF16)

    mixed_ref[0] = turned(0)
    arrival(mix_ref.at[pl.ds(0, 2)], mix_recv.at[1])
    mixed_ref[1] = turned(1)
    mixed_ref[2] = turned(3)

    @pl.loop(0, NX)
    def _(n):
        columns = quarter_of(n)
        part = res_ref[:, columns].astype(F32)
        for m, k in enumerate((0, 1, 3)):
            part = part + nn(mixed_ref[m], wo_ref[lax.rem(x + k, NX), :, columns])
        stream_ref[n] = part

    arrival(mix_ref.at[0], mix_recv.at[0])
    mixed_ref[3] = turned(2)

    def project(n, total):
        part = stream_ref[n] + nn(mixed_ref[3], wo_ref[lax.rem(x + 2, NX), :, quarter_of(n)])
        stream_ref[n] = part
        return total + jnp.sum(part * part, axis=1, keepdims=True)

    square = lax.fori_loop(0, NX, project, jnp.zeros((TOK, 1), F32))
    inverse = lax.rsqrt(square / D + EPSILON)

    @pl.loop(0, NX)
    def _(n):
        columns = quarter_of(n)
        normed_ref[:, columns] = (stream_ref[n] * inverse * egain_ref[:, columns]).astype(BF16)

    @pl.loop(0, NZ)
    def _(i):
        to_z = lax.rem(z + z_offset(i), NZ)
        chosen = pick_ref[pl.ds(pl.multiple_of(to_z * PLANE * CAP, PLANE * CAP), PLANE * CAP)]
        rows = nn(chosen, normed_ref[...])
        sbuf_ref[pl.ds(i * PLANE, PLANE)] = rows.reshape(PLANE, CAP, D).astype(BF16)

        @pl.loop(0, PLANE)
        def _(n):
            to = lax.rem(p + n, PLANE)
            itself = (i == NZ - 1) & (n == 0)

            @pl.when(jnp.logical_not(itself))
            def _():
                pltpu.make_async_remote_copy(
                    sbuf_ref.at[i * PLANE + to],
                    rbuf_ref.at[i * PLANE + p],
                    d_send,
                    d_recv.at[i],
                    device_id=sp_dev(to_z, to),
                    device_id_type=MESH_ID,
                ).start()

            @pl.when(itself)
            def _():
                pltpu.make_async_copy(
                    sbuf_ref.at[i * PLANE + to], rbuf_ref.at[i * PLANE + p], d_recv.at[i]
                ).start()

    arrival(sd_ref.at[pl.ds(0, (NX - 1) * PART)], wrecv_sem.at[3])
    for step in range(1, NX):
        rows = part_rows(lax.rem(x + step, NX))

        @pl.loop(1, PLANE)
        def _(n):
            pltpu.make_async_remote_copy(
                sd_ref.at[rows],
                sd_ref.at[rows],
                swap_send,
                swap_recv,
                device_id=sp_dev(z, lax.rem(p + n, PLANE)),
                device_id_type=MESH_ID,
            ).start()

    for n in range(11, 14):
        loads[n].wait()
    normed = normed_ref[...]
    shared_hidden = jax.nn.silu(nn(normed, sg_ref[...])) * nn(normed, su_ref[...])
    shared_ref[:, own_rows] = shared_hidden.astype(BF16)

    arrival(table_ref.at[pl.ds(0, NZ - 1)], st_recv.at[3])
    slot = lax.broadcasted_iota(jnp.int32, (NEAR, TOK), 0)
    expert = (slot // CAP + z * (PLANE * NX)).astype(F32)
    place = lax.rem(slot, CAP).astype(F32)

    @pl.loop(0, NZ)
    def _(n):
        table = table_ref[n]
        named = jnp.zeros((NEAR, TOK), F32)
        weight = jnp.zeros((NEAR, TOK), F32)
        for k in range(4):
            hit = table[k : k + 1] == expert
            named = jnp.where(hit, 1.0, named)
            weight = jnp.where(hit, table[k + 4 : k + 5], weight)
        rank = nn(named.astype(BF16), strict)
        weight = jnp.transpose(jnp.where(rank == place, weight, 0.0))
        high = weight.astype(BF16)
        whi_ref[n] = high
        wlo_ref[n] = (weight - high.astype(F32)).astype(BF16)

    for cp in own_weights:
        cp.wait()
    arrival(wg_ref.at[:, pl.ds(0, FF - GROUP)], wrecv_sem.at[0])
    arrival(wu_ref.at[:, pl.ds(0, FF - GROUP)], wrecv_sem.at[1])

    def hidden_of(s):
        arrival(rbuf_ref.at[pl.ds(0, PLANE)], d_recv.at[2 * s])
        arrival(rbuf_ref.at[pl.ds(0, PLANE)], d_recv.at[2 * s + 1])
        blocks = pl.ds(pl.multiple_of(s * CHUNK, CHUNK), CHUNK)
        rows = rbuf_ref[blocks].astype(F32).reshape(CHUNK * CAP, D).astype(BF16)
        hidden = jax.nn.silu(nn(rows, wg_ref[...])) * nn(rows, wu_ref[...])
        hidden_ref[s] = hidden.astype(BF16)

    pl.loop(0, NZ // 2 - 1)(hidden_of)

    def send_back(src, dst, sem, columns):
        for j in columns:
            to_x = lax.rem(x + j, NX)

            @pl.loop(0 if j else 1, PLANE)
            def _(n):
                to = lax.rem(p + n, PLANE)
                pltpu.make_async_remote_copy(
                    src(to_x, to),
                    dst,
                    b_send,
                    sem,
                    device_id={**sp_dev(z, to), "tp": to_x},
                    device_id_type=MESH_ID,
                ).start()

            if j == 0:
                pltpu.make_async_copy(src(x, p), dst, sem).start()

    def out_of_expert(s, k, rows, columns):
        for j in columns:
            n = lax.rem(x + j, NX)
            result = nn(rows, wd_ref[:, quarter_of(n)])
            result = result.reshape(-1, PLANE, CAP, QUARTER).astype(BF16)
            for m in range(result.shape[0]):
                eo_ref[s, n, :, k + m] = result[m]

    def one_back(i, columns):
        s, k = i // 2, i % 2
        rows = hidden_ref[s, k * (PLANE * CAP) : (k + 1) * (PLANE * CAP)]
        out_of_expert(s, k, rows, columns)
        send_back(
            lambda to_x, to: eo_ref.at[s, to_x, to, k],
            near_ref.at[s, p * NX + x, k],
            b_recv.at[i],
            columns,
        )

    width = QUARTER // 2

    def weighted(i, h):
        block = lax.rem(z + NZ - z_offset(i), NZ)
        rows = near_ref[i // 2, :, i % 2, :, h * width : (h + 1) * width]
        rows = rows.astype(F32).reshape(NEAR, width).astype(BF16)
        return nn(whi_ref[block], rows) + nn(wlo_ref[block], rows)

    def arrived(i, h):
        arrival(chain_in_ref.at[2 * i + h], chain_recv.at[2 * i + h])
        return chain_in_ref[2 * i + h].astype(F32)

    def passed_on(i, h, before, up):
        part = weighted(i, h)
        if before is not None:
            part = part + arrived(before, h)
        chain_out_ref[2 * i + h] = part.astype(BF16)
        pltpu.make_async_remote_copy(
            chain_out_ref.at[2 * i + h],
            chain_in_ref.at[2 * i + h],
            chain_send,
            chain_recv.at[2 * i + h],
            device_id={"sp_0": lax.rem(z + (1 if up else NZ - 1), NZ)},
            device_id_type=MESH_ID,
        ).start()

    soon, every = (1, 3, 0), (2, 1, 3, 0)

    def returned(i):
        arrival(near_ref.at[i // 2, :, i % 2], b_recv.at[i])

    arrival(wd_ref.at[pl.ds(0, FF - GROUP), pl.ds(0, D - QUARTER)], wrecv_sem.at[2])
    one_back(0, soon)
    hidden_of(NZ // 2 - 1)
    arrival(wd_ref.at[pl.ds(0, FF - GROUP), pl.ds(0, QUARTER)], wrecv_sem.at[4])
    one_back(0, (2,))
    one_back(1, every)
    one_back(2, every)
    one_back(3, every)
    returned(0)
    passed_on(0, 0, None, True)
    passed_on(0, 1, None, False)
    one_back(4, every)
    returned(1)
    passed_on(1, 0, None, False)
    one_back(5, every)
    returned(2)
    passed_on(2, 1, None, True)
    passed_on(2, 0, 0, True)
    passed_on(1, 1, 0, False)
    one_back(6, every)
    returned(3)
    passed_on(3, 0, 1, False)
    one_back(7, every)
    for step in (2, 1, 3):
        pltpu.make_async_remote_copy(
            shared_ref.at[:, own_rows],
            shared_ref.at[:, own_rows],
            rs_ssem,
            rs_rsem,
            device_id={"tp": lax.rem(x + step, NX)},
            device_id_type=MESH_ID,
        ).start()
    returned(4)
    passed_on(4, 1, 2, True)
    passed_on(3, 1, 1, False)
    passed_on(4, 0, 2, True)
    returned(5)
    passed_on(5, 0, 3, False)
    returned(6)
    passed_on(6, 1, 4, True)
    passed_on(5, 1, 3, False)
    passed_on(6, 0, 4, True)

    arrival(near_ref.at[3, :, 1], b_recv.at[7])
    totals = []
    for h in range(2):
        totals.append(stream_ref[x, :, h * width : (h + 1) * width] + weighted(NZ - 1, h))
    arrival(sd_ref.at[pl.ds(0, (NX - 1) * (GROUP - PART))], swap_recv)
    arrival(shared_ref.at[:, pl.ds(0, FF - GROUP)], rs_rsem)
    for h in (1, 0):
        columns = slice(h * width, (h + 1) * width)
        total = totals[h] + nn(shared_ref[...], sd_ref[:, columns])
        total = total + arrived(5, h) + arrived(6, h)
        out_ref[:, columns] = total.astype(BF16)

    arrival(plane_ref.at[pl.ds(0, PLANE - 1)], st_send.at[0])
    arrival(zst_ref.at[pl.ds(0, NZ - 1)], st_send.at[1])
    arrival(fin_ref.at[pl.ds(0, PLANE - 1)], st_send.at[2])
    arrival(mix_ref.at[pl.ds(0, NX - 1)], mix_send)
    arrival(wg_ref.at[:, pl.ds(0, FF - GROUP)], wsend_sem.at[0])
    arrival(wu_ref.at[:, pl.ds(0, FF - GROUP)], wsend_sem.at[1])
    arrival(wd_ref.at[pl.ds(0, FF - GROUP)], wsend_sem.at[2])
    arrival(sbuf_ref.at[pl.ds(0, N_SP - 1)], d_send)
    arrival(table_ref.at[pl.ds(0, NZ - 1)], st_send.at[3])
    for n in range(NZ // 2):
        arrival(near_ref.at[n, pl.ds(0, NX * PLANE - 1)], b_send)
    arrival(sd_ref.at[pl.ds(0, (NX - 1) * PART)], wsend_sem.at[3])
    arrival(sd_ref.at[pl.ds(0, (NX - 1) * (GROUP - PART))], swap_send)
    arrival(shared_ref.at[:, pl.ds(0, FF - GROUP)], rs_ssem)
    arrival(chain_out_ref, chain_send)


def body(
    memory_queries,
    memory_keys,
    memory_values,
    output_gate_preactivation,
    log_input_gate,
    forget_preactivation,
    head_forget_bias,
    forget_extra_boost,
    head_norm_gain,
    memory_output_weight,
    residual,
    expert_norm_gain,
    routes,
    router_weight_matrix,
    routed_gate_weight,
    routed_up_weight,
    routed_down_weight,
    shared_gate_weight,
    shared_up_weight,
    shared_down_weight,
):
    anywhere = pl.BlockSpec(memory_space=pl.ANY)
    vmem = pl.BlockSpec(memory_space=pltpu.VMEM)
    smem = pl.BlockSpec(memory_space=pltpu.SMEM)
    specs = [anywhere] * 20
    specs[6] = smem
    specs[8] = vmem
    specs[11] = vmem
    dma = pltpu.SemaphoreType.DMA
    return pl.pallas_call(
        kernel,
        out_shape=jax.ShapeDtypeStruct((TOK, QUARTER), BF16),
        in_specs=specs,
        out_specs=vmem,
        scratch_shapes=[
            pltpu.VMEM((HW, TOK), BF16),
            pltpu.VMEM((HW, TOK), BF16),
            pltpu.VMEM((HW, TOK), BF16),
            pltpu.VMEM((HW, TOK), BF16),
            pltpu.VMEM((2, TOK), F32),
            pltpu.VMEM((2, TOK), F32),
            pltpu.VMEM((2, TOK), F32),
            pltpu.VMEM((NX, HW, D), BF16),
            pltpu.VMEM((TOK, D), BF16),
            pltpu.VMEM((4, TOK), jnp.int32),
            pltpu.VMEM((4, TOK), F32),
            pltpu.VMEM((D, GROUP), BF16),
            pltpu.VMEM((D, GROUP), BF16),
            pltpu.VMEM((FF, QUARTER), BF16),
            pltpu.VMEM((D, FF), BF16),
            pltpu.VMEM((D, FF), BF16),
            pltpu.VMEM((FF, D), BF16),
            pltpu.VMEM((PLANE, SLICE, LANES), F32),
            pltpu.VMEM((PLANE, SLICE, LANES), F32),
            pltpu.VMEM((NZ, SLICE, LANES), F32),
            pltpu.VMEM((PLANE, SLICE, LANES), F32),
            pltpu.VMEM((PLANE, SLICE, LANES), F32),
            pltpu.VMEM((NX, HW, TOK), BF16),
            pltpu.VMEM((NX, TOK, HW), BF16),
            pltpu.VMEM((NZ // 2, CHUNK * CAP, FF), BF16),
            pltpu.VMEM((NX, TOK, QUARTER), F32),
            pltpu.VMEM((TOK, D), BF16),
            pltpu.VMEM((SLOTS, TOK), BF16),
            pltpu.VMEM((NZ, TOK, NEAR), BF16),
            pltpu.VMEM((NZ, TOK, NEAR), BF16),
            pltpu.VMEM((TOK, FF), BF16),
            pltpu.VMEM((N_SP, CAP, D), BF16),
            pltpu.VMEM((N_SP, CAP, D), BF16),
            pltpu.VMEM((NZ // 2, NX, PLANE, 2, CAP, QUARTER), BF16),
            pltpu.VMEM((NZ // 2, NX * PLANE, 2, CAP, QUARTER), BF16),
            pltpu.VMEM((14, TOK, QUARTER // 2), BF16),
            pltpu.VMEM((14, TOK, QUARTER // 2), BF16),
            pltpu.VMEM((NZ, 8, TOK), F32),
            dma((14,)),
            dma((3,)),
            dma((4,)),
            dma((5,)),
            dma((4,)),
            dma((4,)),
            dma,
            dma((2,)),
            dma,
            dma((NZ,)),
            dma,
            dma((NZ,)),
            dma,
            dma,
            dma,
            dma((14,)),
            dma,
            dma,
        ],
        compiler_params=pltpu.CompilerParams(
            collective_id=0, has_side_effects=True, vmem_limit_bytes=60 << 20
        ),
        name="layer",
    )(
        memory_queries.T,
        memory_keys.T,
        memory_values.T,
        output_gate_preactivation.T,
        log_input_gate,
        forget_preactivation,
        head_forget_bias,
        forget_extra_boost,
        head_norm_gain.reshape(1, HW),
        memory_output_weight.reshape(NX, HW, D),
        residual,
        expert_norm_gain.reshape(1, D),
        routes.T,
        router_weight_matrix.T,
        routed_gate_weight,
        routed_up_weight,
        routed_down_weight,
        shared_gate_weight,
        shared_up_weight,
        shared_down_weight,
    )


def solution(mesh):
    split = Mesh(
        mesh.devices.reshape(NZ, NY, NC, mesh.shape["tp"]), ("sp_0", "sp_1", "sp_2", "tp")
    )
    return jax.shard_map(
        body,
        mesh=split,
        in_specs=(
            P(SP, "tp"),
            P(SP, "tp"),
            P(SP, "tp"),
            P(SP, "tp"),
            P("tp", SP),
            P("tp", SP),
            P("tp"),
            P("tp", SP),
            P("tp"),
            P(),
            P(SP, None),
            P(),
            P(SP, None),
            P(SP, None),
            P(SP, None, "tp"),
            P(SP, None, "tp"),
            P(SP, "tp", None),
            P(None, "tp"),
            P(None, "tp"),
            P("tp", None),
        ),
        out_specs=P(SP, "tp"),
        check_vma=False,
    )
```

```python
import jax
import jax.numpy as jnp
from jax import lax
from jax.experimental import pallas as pl
from jax.experimental.pallas import tpu as pltpu
from jax.sharding import Mesh
from jax.sharding import PartitionSpec as P

SP = ("sp_0", "sp_1", "sp_2")
MESH_ID = pl.DeviceIdType.MESH
NEG_LARGE = -1e30
EPSILON = 1e-06
F32 = jnp.float32
BF16 = jnp.bfloat16
HIGHEST = lax.Precision.HIGHEST

NZ, NY, NC, NX = 8, 4, 2, 4
PLANE = NY * NC
N_SP = NZ * PLANE
TOK = 256
DH = 96
HW = 192
D = 2048
FF = 512
GROUP = FF // NX
PART = GROUP // PLANE
CAP = 8
SLOTS = N_SP * CAP
NEAR = PLANE * NX * CAP
LANES = 128
SOON = 1280
SLICE = HW // PLANE
QUARTER = D // NX
CHUNK = 2 * PLANE


def nt(a, b, precision=None):
    return lax.dot_general(
        a, b, (((1,), (1,)), ((), ())), preferred_element_type=F32, precision=precision
    )


def tn(a, b, precision=None):
    return lax.dot_general(
        a, b, (((0,), (0,)), ((), ())), preferred_element_type=F32, precision=precision
    )


def nn(a, b, precision=None):
    return jnp.dot(a, b, preferred_element_type=F32, precision=precision)


def arrival(ref, sem):
    pltpu.make_async_copy(ref, ref, sem).wait()


def z_offset(i):
    return jnp.where(lax.rem(i, 2) == 0, 4 + i // 2, 4 - (i + 1) // 2)


def kernel(
    q_hbm,
    k_hbm,
    v_hbm,
    og_hbm,
    lig_hbm,
    fpre_hbm,
    bias_ref,
    boost_hbm,
    hgain_ref,
    wo_hbm,
    res_hbm,
    egain_ref,
    routes_hbm,
    rw_hbm,
    gate_hbm,
    up_hbm,
    down_hbm,
    sg_hbm,
    su_hbm,
    sd_hbm,
    out_ref,
    q_ref,
    k_ref,
    v_ref,
    og_ref,
    lig_ref,
    fpre_ref,
    boost_ref,
    wo_ref,
    res_ref,
    routes_ref,
    rw_ref,
    sg_ref,
    su_ref,
    sd_ref,
    wg_ref,
    wu_ref,
    wd_ref,
    state_ref,
    plane_ref,
    zst_ref,
    fin_ref,
    carry_ref,
    mix_ref,
    mixed_ref,
    hidden_ref,
    stream_ref,
    normed_ref,
    pick_ref,
    whi_ref,
    wlo_ref,
    shared_ref,
    sbuf_ref,
    rbuf_ref,
    eo_ref,
    near_ref,
    chain_out_ref,
    chain_in_ref,
    table_ref,
    in_sem,
    own_sem,
    wsend_sem,
    wrecv_sem,
    st_send,
    st_recv,
    mix_send,
    mix_recv,
    d_send,
    d_recv,
    b_send,
    b_recv,
    rs_ssem,
    rs_rsem,
    chain_send,
    chain_recv,
    swap_send,
    swap_recv,
):
    z, y, c, x = (lax.axis_index(a) for a in ("sp_0", "sp_1", "sp_2", "tp"))
    p = y * NC + c
    sp = z * PLANE + p

    def sp_dev(tz, tp_):
        return {"sp_0": tz, "sp_1": tp_ // NC, "sp_2": lax.rem(tp_, NC)}

    own_rows = pl.ds(pl.multiple_of(x * GROUP, GROUP), GROUP)

    def quarter_of(n):
        return pl.ds(pl.multiple_of(n * QUARTER, QUARTER), QUARTER)

    early = (
        (lig_hbm, lig_ref),
        (fpre_hbm, fpre_ref),
        (boost_hbm, boost_ref),
        (k_hbm, k_ref),
        (v_hbm, v_ref),
        (q_hbm, q_ref),
        (og_hbm, og_ref),
        (routes_hbm, routes_ref),
        (rw_hbm, rw_ref),
        (wo_hbm, wo_ref),
        (res_hbm, res_ref),
        (sg_hbm, sg_ref),
        (su_hbm, su_ref),
        (sd_hbm.at[:, quarter_of(x)], sd_ref.at[own_rows]),
    )
    loads = [pltpu.make_async_copy(a, b, in_sem.at[n]) for n, (a, b) in enumerate(early)]
    for cp in loads:
        cp.start()

    barrier = pltpu.get_barrier_semaphore()

    @pl.loop(1, NZ)
    def _(n):
        pl.semaphore_signal(
            barrier, inc=1, device_id={"sp_0": lax.rem(z + n, NZ)}, device_id_type=MESH_ID
        )

    @pl.loop(1, PLANE)
    def _(n):
        pl.semaphore_signal(
            barrier, inc=1, device_id=sp_dev(z, lax.rem(p + n, PLANE)), device_id_type=MESH_ID
        )

    for n in range(1, NX):
        pl.semaphore_signal(
            barrier, inc=1, device_id={"tp": lax.rem(x + n, NX)}, device_id_type=MESH_ID
        )

    own_weights = (
        pltpu.make_async_copy(
            gate_hbm.at[x], wg_ref.at[:, own_rows], own_sem.at[0]
        ),
        pltpu.make_async_copy(
            up_hbm.at[x], wu_ref.at[:, own_rows], own_sem.at[1]
        ),
        pltpu.make_async_copy(
            down_hbm.at[x], wd_ref.at[own_rows], own_sem.at[2]
        ),
    )

    for n in range(3):
        loads[n].wait()
    second = lax.broadcasted_iota(jnp.int32, (2, TOK), 0) == 1
    bias = jnp.where(second, bias_ref[1], bias_ref[0])
    pre = fpre_ref[...] + bias
    log_forget = jnp.minimum(pre, 0.0) - jnp.log1p(jnp.exp(-jnp.abs(pre))) + boost_ref[...]
    row = lax.broadcasted_iota(jnp.int32, (TOK, TOK), 0)
    col = lax.broadcasted_iota(jnp.int32, (TOK, TOK), 1)
    causal = row <= col
    upper = jnp.where(causal, 1.0, 0.0).astype(F32)
    eye = jnp.where(row == col, 1.0, 0.0).astype(F32)
    log_in = lig_ref[...]
    cumul = nn(log_forget, upper, HIGHEST)
    source = nt(eye, log_in - cumul, HIGHEST)
    ending = jnp.sum(log_forget, axis=1, keepdims=True)
    w_log = ending - cumul + log_in
    local_top = jnp.max(w_log, axis=1, keepdims=True)
    w_end = jnp.exp(w_log - local_top)

    loads[3].wait()
    loads[4].wait()
    lane = lax.broadcasted_iota(jnp.int32, (DH, LANES), 1)
    slice_lane = lax.broadcasted_iota(jnp.int32, (SLICE, LANES), 1)

    def with_scalars(mem, top, total, lanes):
        return jnp.where(lanes == DH, top, jnp.where(lanes == DH + 1, total, mem))

    def taken_apart(block):
        return block, block[:, DH : DH + 1], block[:, DH + 1 : DH + 2]

    padding = jnp.zeros((LANES - DH, TOK), F32)
    for h in range(2):
        keys = k_ref[h * DH : (h + 1) * DH].astype(F32) * w_end[h : h + 1]
        values = v_ref[h * DH : (h + 1) * DH].astype(F32)
        memory = nt(values, jnp.concatenate([keys, padding], axis=0), HIGHEST)
        state = with_scalars(memory, local_top[h : h + 1], ending[h : h + 1], lane)
        state_ref[h * (PLANE // 2) : (h + 1) * (PLANE // 2)] = state.reshape(PLANE // 2, SLICE, LANES)

    pl.semaphore_wait(barrier, NZ - 1 + PLANE - 1 + NX - 1)

    @pl.loop(1, PLANE)
    def _(n):
        to = lax.rem(p + n, PLANE)
        pltpu.make_async_remote_copy(
            state_ref.at[to],
            plane_ref.at[p],
            st_send.at[0],
            st_recv.at[0],
            device_id=sp_dev(z, to),
            device_id_type=MESH_ID,
        ).start()

    def send_weights(n, src, dst):
        for step in (2, 1, 3):
            to = lax.rem(x + step, NX)
            pltpu.make_async_remote_copy(
                src(to),
                dst,
                wsend_sem.at[n],
                wrecv_sem.at[n],
                device_id={"tp": to},
                device_id_type=MESH_ID,
            ).start()

    upper_half, lower_half = pl.ds(0, SOON), pl.ds(SOON, D - SOON)
    def part_rows(k):
        return pl.ds(pl.multiple_of(k * GROUP + p * PART, PART), PART)

    send_weights(
        3,
        lambda to: sd_hbm.at[
            pl.ds(pl.multiple_of(p * PART, PART), PART),
            quarter_of(to),
        ],
        sd_ref.at[part_rows(x)],
    )
    send_weights(0, lambda to: gate_hbm.at[to, upper_half], wg_ref.at[upper_half, own_rows])
    for cp in own_weights:
        cp.start()
    plane_ref[p] = state_ref[p]

    loads[5].wait()
    scale = DH ** (-0.5)
    local_max, numer = [], []
    for h in range(2):
        head = slice(h * DH, (h + 1) * DH)
        d_log = jnp.where(causal, cumul[h : h + 1] + source[:, h : h + 1], NEG_LARGE)
        top = jnp.max(d_log, axis=0, keepdims=True)
        scores = tn(k_ref[head], q_ref[head]) * scale
        within = (scores * jnp.exp(d_log - top)).astype(BF16)
        numer.append(nn(v_ref[head], within))
        local_max.append(top)

    def join(earlier, later):
        mem_a, top_a, total_a = earlier
        mem_b, top_b, total_b = later
        top = jnp.maximum(total_b + top_a, top_b)
        mem = jnp.exp(total_b + top_a - top) * mem_a + jnp.exp(top_b - top) * mem_b
        return mem, top, total_a + total_b

    none = (
        jnp.zeros((SLICE, LANES), F32),
        jnp.full((SLICE, 1), NEG_LARGE, F32),
        jnp.zeros((SLICE, 1), F32),
    )
    arrival(plane_ref.at[pl.ds(0, PLANE - 1)], st_recv.at[0])
    whole, before = none, []
    for n in range(PLANE):
        before.append(whole)
        whole = join(whole, taken_apart(plane_ref[n]))
    zst_ref[z] = with_scalars(*whole, slice_lane)

    @pl.loop(1, NZ)
    def _(n):
        pltpu.make_async_remote_copy(
            zst_ref.at[z],
            zst_ref.at[z],
            st_send.at[1],
            st_recv.at[1],
            device_id={"sp_0": lax.rem(z + n, NZ)},
            device_id_type=MESH_ID,
        ).start()

    loads[7].wait()
    loads[8].wait()
    table_ref[z] = jnp.concatenate([routes_ref[...].astype(F32), rw_ref[...]], axis=0)

    @pl.loop(1, NZ)
    def _(n):
        pltpu.make_async_remote_copy(
            table_ref.at[z],
            table_ref.at[z],
            st_send.at[3],
            st_recv.at[3],
            device_id={"sp_0": lax.rem(z + n, NZ)},
            device_id_type=MESH_ID,
        ).start()

    slot = lax.broadcasted_iota(jnp.int32, (SLOTS, TOK), 0)
    expert = slot // CAP * NX + x
    named = jnp.zeros((SLOTS, TOK), F32)
    for n in range(4):
        named = jnp.where(routes_ref[n : n + 1] == expert, 1.0, named)
    strict = jnp.where(row < col, 1.0, 0.0).astype(BF16)
    rank = nn(named.astype(BF16), strict)
    pick_ref[...] = jnp.where(rank == lax.rem(slot, CAP).astype(F32), named, 0.0).astype(BF16)
    hgain = nt(eye[:HW, :HW], hgain_ref[...], HIGHEST)
    loads[6].wait()
    gating = hgain * jax.nn.sigmoid(og_ref[...].astype(F32))

    arrival(zst_ref.at[pl.ds(0, NZ - 1)], st_recv.at[1])
    carried = none
    for n in range(NZ):
        mem, top, total = taken_apart(zst_ref[n])
        passed = n < z
        carried = join(
            carried, (mem, jnp.where(passed, top, NEG_LARGE), jnp.where(passed, total, 0.0))
        )
    z_mem, z_top, z_total = carried
    z_mem = jnp.where(z > 0, z_mem, 0.0)
    for n in range(PLANE):
        fin_ref[n] = with_scalars(*join((z_mem, z_top, z_total), before[n]), slice_lane)

    @pl.loop(1, PLANE)
    def _(n):
        to = lax.rem(p + n, PLANE)
        pltpu.make_async_remote_copy(
            fin_ref.at[to],
            carry_ref.at[p],
            st_send.at[2],
            st_recv.at[2],
            device_id=sp_dev(z, to),
            device_id_type=MESH_ID,
        ).start()

    carry_ref[p] = fin_ref[p]
    arrival(carry_ref.at[pl.ds(0, PLANE - 1)], st_recv.at[2])
    no_queries = jnp.zeros((LANES - DH, TOK), BF16)
    for h in range(2):
        head = slice(h * DH, (h + 1) * DH)
        memory = carry_ref[h * (PLANE // 2) : (h + 1) * (PLANE // 2)].reshape(DH, LANES)
        carry_top = memory[0:1, DH : DH + 1]
        memory = jnp.where(lane < DH, memory, 0.0)
        high = memory.astype(BF16)
        low = (memory - high.astype(F32)).astype(BF16)
        queries = jnp.concatenate([q_ref[head], no_queries], axis=0)
        inter = nn(high, queries) + nn(low, queries)
        g_log = cumul[h : h + 1] + carry_top
        stab = jnp.maximum(g_log, local_max[h])
        cell = numer[h] * jnp.exp(local_max[h] - stab) + inter * (jnp.exp(g_log - stab) * scale)
        mean = jnp.sum(cell * cell, axis=0, keepdims=True) / DH
        mix_ref[x, head] = (cell * lax.rsqrt(mean + EPSILON) * gating[head]).astype(BF16)
    for step in (1, 3, 2):
        pltpu.make_async_remote_copy(
            mix_ref.at[x],
            mix_ref.at[x],
            mix_send,
            mix_recv.at[step % 2],
            device_id={"tp": lax.rem(x + step, NX)},
            device_id_type=MESH_ID,
        ).start()
    send_weights(0, lambda to: gate_hbm.at[to, lower_half], wg_ref.at[lower_half, own_rows])
    send_weights(1, lambda to: up_hbm.at[to], wu_ref.at[:, own_rows])
    for j in (0, 1, 3, 2):
        for step in (2, 1, 3):
            to = lax.rem(x + step, NX)
            columns = quarter_of(lax.rem(to + j, NX))
            pltpu.make_async_remote_copy(
                down_hbm.at[to, :, columns],
                wd_ref.at[own_rows, columns],
                wsend_sem.at[2],
                wrecv_sem.at[4 if j == 2 else 2],
                device_id={"tp": to},
                device_id_type=MESH_ID,
            ).start()

    loads[9].wait()
    loads[10].wait()

    def turned(k):
        return jnp.transpose(mix_ref[lax.rem(x + k, NX)].astype(F32)).astype(BF16)

    mixed_ref[0] = turned(0)

    @pl.loop(0, NX)
    def _(n):
        columns = quarter_of(n)
        stream_ref[n] = res_ref[:, columns].astype(F32) + nn(mixed_ref[0], wo_ref[x, :, columns])

    arrival(mix_ref.at[pl.ds(0, 2)], mix_recv.at[1])
    arrival(mix_ref.at[0], mix_recv.at[0])
    for k in range(1, NX):
        mixed_ref[k] = turned(k)

    def project(n, total):
        part = stream_ref[n]
        for k in range(1, NX):
            part = part + nn(mixed_ref[k], wo_ref[lax.rem(x + k, NX), :, quarter_of(n)])
        stream_ref[n] = part
        return total + jnp.sum(part * part, axis=1, keepdims=True)

    square = lax.fori_loop(0, NX, project, jnp.zeros((TOK, 1), F32))
    inverse = lax.rsqrt(square / D + EPSILON)

    @pl.loop(0, NX)
    def _(n):
        columns = quarter_of(n)
        normed_ref[:, columns] = (stream_ref[n] * inverse * egain_ref[:, columns]).astype(BF16)

    @pl.loop(0, NZ)
    def _(i):
        to_z = lax.rem(z + z_offset(i), NZ)
        chosen = pick_ref[pl.ds(pl.multiple_of(to_z * PLANE * CAP, PLANE * CAP), PLANE * CAP)]
        rows = nn(chosen, normed_ref[...])
        sbuf_ref[pl.ds(i * PLANE, PLANE)] = rows.reshape(PLANE, CAP, D).astype(BF16)

        @pl.loop(0, PLANE)
        def _(n):
            to = lax.rem(p + n, PLANE)
            itself = (i == NZ - 1) & (n == 0)

            @pl.when(jnp.logical_not(itself))
            def _():
                pltpu.make_async_remote_copy(
                    sbuf_ref.at[i * PLANE + to],
                    rbuf_ref.at[i * PLANE + p],
                    d_send,
                    d_recv.at[i],
                    device_id=sp_dev(to_z, to),
                    device_id_type=MESH_ID,
                ).start()

            @pl.when(itself)
            def _():
                pltpu.make_async_copy(
                    sbuf_ref.at[i * PLANE + to], rbuf_ref.at[i * PLANE + p], d_recv.at[i]
                ).start()

    arrival(sd_ref.at[pl.ds(0, (NX - 1) * PART)], wrecv_sem.at[3])
    for step in range(1, NX):
        rows = part_rows(lax.rem(x + step, NX))

        @pl.loop(1, PLANE)
        def _(n):
            pltpu.make_async_remote_copy(
                sd_ref.at[rows],
                sd_ref.at[rows],
                swap_send,
                swap_recv,
                device_id=sp_dev(z, lax.rem(p + n, PLANE)),
                device_id_type=MESH_ID,
            ).start()

    for n in range(11, 14):
        loads[n].wait()
    normed = normed_ref[...]
    shared_hidden = jax.nn.silu(nn(normed, sg_ref[...])) * nn(normed, su_ref[...])
    shared_ref[:, own_rows] = shared_hidden.astype(BF16)

    arrival(table_ref.at[pl.ds(0, NZ - 1)], st_recv.at[3])
    slot = lax.broadcasted_iota(jnp.int32, (NEAR, TOK), 0)
    expert = (slot // CAP + z * (PLANE * NX)).astype(F32)
    place = lax.rem(slot, CAP).astype(F32)

    @pl.loop(0, NZ)
    def _(n):
        table = table_ref[n]
        named = jnp.zeros((NEAR, TOK), F32)
        weight = jnp.zeros((NEAR, TOK), F32)
        for k in range(4):
            hit = table[k : k + 1] == expert
            named = jnp.where(hit, 1.0, named)
            weight = jnp.where(hit, table[k + 4 : k + 5], weight)
        rank = nn(named.astype(BF16), strict)
        weight = jnp.transpose(jnp.where(rank == place, weight, 0.0))
        high = weight.astype(BF16)
        whi_ref[n] = high
        wlo_ref[n] = (weight - high.astype(F32)).astype(BF16)

    for cp in own_weights:
        cp.wait()
    arrival(wg_ref.at[:, pl.ds(0, FF - GROUP)], wrecv_sem.at[0])
    arrival(wu_ref.at[:, pl.ds(0, FF - GROUP)], wrecv_sem.at[1])

    def hidden_of(s):
        arrival(rbuf_ref.at[pl.ds(0, PLANE)], d_recv.at[2 * s])
        arrival(rbuf_ref.at[pl.ds(0, PLANE)], d_recv.at[2 * s + 1])
        blocks = pl.ds(pl.multiple_of(s * CHUNK, CHUNK), CHUNK)
        rows = rbuf_ref[blocks].astype(F32).reshape(CHUNK * CAP, D).astype(BF16)
        hidden = jax.nn.silu(nn(rows, wg_ref[...])) * nn(rows, wu_ref[...])
        hidden_ref[s] = hidden.astype(BF16)

    pl.loop(0, NZ // 2 - 1)(hidden_of)

    def send_back(src, dst, sem, columns):
        for j in columns:
            to_x = lax.rem(x + j, NX)

            @pl.loop(0 if j else 1, PLANE)
            def _(n):
                to = lax.rem(p + n, PLANE)
                pltpu.make_async_remote_copy(
                    src(to_x, to),
                    dst,
                    b_send,
                    sem,
                    device_id={**sp_dev(z, to), "tp": to_x},
                    device_id_type=MESH_ID,
                ).start()

            if j == 0:
                pltpu.make_async_copy(src(x, p), dst, sem).start()

    def out_of_expert(s, k, rows, columns):
        for j in columns:
            n = lax.rem(x + j, NX)
            result = nn(rows, wd_ref[:, quarter_of(n)])
            result = result.reshape(-1, PLANE, CAP, QUARTER).astype(BF16)
            for m in range(result.shape[0]):
                eo_ref[s, n, :, k + m] = result[m]

    def one_back(i, columns):
        s, k = i // 2, i % 2
        rows = hidden_ref[s, k * (PLANE * CAP) : (k + 1) * (PLANE * CAP)]
        out_of_expert(s, k, rows, columns)
        send_back(
            lambda to_x, to: eo_ref.at[s, to_x, to, k],
            near_ref.at[s, p * NX + x, k],
            b_recv.at[i],
            columns,
        )

    width = QUARTER // 2

    def weighted(i, h):
        block = lax.rem(z + NZ - z_offset(i), NZ)
        rows = near_ref[i // 2, :, i % 2, :, h * width : (h + 1) * width]
        rows = rows.astype(F32).reshape(NEAR, width).astype(BF16)
        return nn(whi_ref[block], rows) + nn(wlo_ref[block], rows)

    def arrived(i, h):
        arrival(chain_in_ref.at[2 * i + h], chain_recv.at[2 * i + h])
        return chain_in_ref[2 * i + h].astype(F32)

    def passed_on(i, h, before, up):
        part = weighted(i, h)
        if before is not None:
            part = part + arrived(before, h)
        chain_out_ref[2 * i + h] = part.astype(BF16)
        pltpu.make_async_remote_copy(
            chain_out_ref.at[2 * i + h],
            chain_in_ref.at[2 * i + h],
            chain_send,
            chain_recv.at[2 * i + h],
            device_id={"sp_0": lax.rem(z + (1 if up else NZ - 1), NZ)},
            device_id_type=MESH_ID,
        ).start()

    soon, every = (1, 3, 0), (2, 1, 3, 0)

    def returned(i):
        arrival(near_ref.at[i // 2, :, i % 2], b_recv.at[i])

    arrival(wd_ref.at[pl.ds(0, FF - GROUP), pl.ds(0, D - QUARTER)], wrecv_sem.at[2])
    one_back(0, soon)
    hidden_of(NZ // 2 - 1)
    arrival(wd_ref.at[pl.ds(0, FF - GROUP), pl.ds(0, QUARTER)], wrecv_sem.at[4])
    one_back(0, (2,))
    one_back(1, every)
    one_back(2, every)
    one_back(3, every)
    returned(0)
    passed_on(0, 0, None, True)
    passed_on(0, 1, None, False)
    one_back(4, every)
    returned(1)
    passed_on(1, 0, None, False)
    one_back(5, every)
    returned(2)
    passed_on(2, 1, None, True)
    passed_on(2, 0, 0, True)
    passed_on(1, 1, 0, False)
    one_back(6, every)
    returned(3)
    passed_on(3, 0, 1, False)
    one_back(7, every)
    for step in (2, 1, 3):
        pltpu.make_async_remote_copy(
            shared_ref.at[:, own_rows],
            shared_ref.at[:, own_rows],
            rs_ssem,
            rs_rsem,
            device_id={"tp": lax.rem(x + step, NX)},
            device_id_type=MESH_ID,
        ).start()
    returned(4)
    passed_on(4, 1, 2, True)
    passed_on(3, 1, 1, False)
    passed_on(4, 0, 2, True)
    returned(5)
    passed_on(5, 0, 3, False)
    returned(6)
    passed_on(6, 1, 4, True)
    passed_on(5, 1, 3, False)
    passed_on(6, 0, 4, True)

    arrival(near_ref.at[3, :, 1], b_recv.at[7])
    totals = []
    for h in range(2):
        totals.append(stream_ref[x, :, h * width : (h + 1) * width] + weighted(NZ - 1, h))
    arrival(sd_ref.at[pl.ds(0, (NX - 1) * (GROUP - PART))], swap_recv)
    arrival(shared_ref.at[:, pl.ds(0, FF - GROUP)], rs_rsem)
    for h in (1, 0):
        columns = slice(h * width, (h + 1) * width)
        total = totals[h] + nn(shared_ref[...], sd_ref[:, columns])
        total = total + arrived(5, h) + arrived(6, h)
        out_ref[:, columns] = total.astype(BF16)

    arrival(plane_ref.at[pl.ds(0, PLANE - 1)], st_send.at[0])
    arrival(zst_ref.at[pl.ds(0, NZ - 1)], st_send.at[1])
    arrival(fin_ref.at[pl.ds(0, PLANE - 1)], st_send.at[2])
    arrival(mix_ref.at[pl.ds(0, NX - 1)], mix_send)
    arrival(wg_ref.at[:, pl.ds(0, FF - GROUP)], wsend_sem.at[0])
    arrival(wu_ref.at[:, pl.ds(0, FF - GROUP)], wsend_sem.at[1])
    arrival(wd_ref.at[pl.ds(0, FF - GROUP)], wsend_sem.at[2])
    arrival(sbuf_ref.at[pl.ds(0, N_SP - 1)], d_send)
    arrival(table_ref.at[pl.ds(0, NZ - 1)], st_send.at[3])
    for n in range(NZ // 2):
        arrival(near_ref.at[n, pl.ds(0, NX * PLANE - 1)], b_send)
    arrival(sd_ref.at[pl.ds(0, (NX - 1) * PART)], wsend_sem.at[3])
    arrival(sd_ref.at[pl.ds(0, (NX - 1) * (GROUP - PART))], swap_send)
    arrival(shared_ref.at[:, pl.ds(0, FF - GROUP)], rs_ssem)
    arrival(chain_out_ref, chain_send)


def body(
    memory_queries,
    memory_keys,
    memory_values,
    output_gate_preactivation,
    log_input_gate,
    forget_preactivation,
    head_forget_bias,
    forget_extra_boost,
    head_norm_gain,
    memory_output_weight,
    residual,
    expert_norm_gain,
    routes,
    router_weight_matrix,
    routed_gate_weight,
    routed_up_weight,
    routed_down_weight,
    shared_gate_weight,
    shared_up_weight,
    shared_down_weight,
):
    anywhere = pl.BlockSpec(memory_space=pl.ANY)
    vmem = pl.BlockSpec(memory_space=pltpu.VMEM)
    smem = pl.BlockSpec(memory_space=pltpu.SMEM)
    specs = [anywhere] * 20
    specs[6] = smem
    specs[8] = vmem
    specs[11] = vmem
    dma = pltpu.SemaphoreType.DMA
    return pl.pallas_call(
        kernel,
        out_shape=jax.ShapeDtypeStruct((TOK, QUARTER), BF16),
        in_specs=specs,
        out_specs=vmem,
        scratch_shapes=[
            pltpu.VMEM((HW, TOK), BF16),
            pltpu.VMEM((HW, TOK), BF16),
            pltpu.VMEM((HW, TOK), BF16),
            pltpu.VMEM((HW, TOK), BF16),
            pltpu.VMEM((2, TOK), F32),
            pltpu.VMEM((2, TOK), F32),
            pltpu.VMEM((2, TOK), F32),
            pltpu.VMEM((NX, HW, D), BF16),
            pltpu.VMEM((TOK, D), BF16),
            pltpu.VMEM((4, TOK), jnp.int32),
            pltpu.VMEM((4, TOK), F32),
            pltpu.VMEM((D, GROUP), BF16),
            pltpu.VMEM((D, GROUP), BF16),
            pltpu.VMEM((FF, QUARTER), BF16),
            pltpu.VMEM((D, FF), BF16),
            pltpu.VMEM((D, FF), BF16),
            pltpu.VMEM((FF, D), BF16),
            pltpu.VMEM((PLANE, SLICE, LANES), F32),
            pltpu.VMEM((PLANE, SLICE, LANES), F32),
            pltpu.VMEM((NZ, SLICE, LANES), F32),
            pltpu.VMEM((PLANE, SLICE, LANES), F32),
            pltpu.VMEM((PLANE, SLICE, LANES), F32),
            pltpu.VMEM((NX, HW, TOK), BF16),
            pltpu.VMEM((NX, TOK, HW), BF16),
            pltpu.VMEM((NZ // 2, CHUNK * CAP, FF), BF16),
            pltpu.VMEM((NX, TOK, QUARTER), F32),
            pltpu.VMEM((TOK, D), BF16),
            pltpu.VMEM((SLOTS, TOK), BF16),
            pltpu.VMEM((NZ, TOK, NEAR), BF16),
            pltpu.VMEM((NZ, TOK, NEAR), BF16),
            pltpu.VMEM((TOK, FF), BF16),
            pltpu.VMEM((N_SP, CAP, D), BF16),
            pltpu.VMEM((N_SP, CAP, D), BF16),
            pltpu.VMEM((NZ // 2, NX, PLANE, 2, CAP, QUARTER), BF16),
            pltpu.VMEM((NZ // 2, NX * PLANE, 2, CAP, QUARTER), BF16),
            pltpu.VMEM((14, TOK, QUARTER // 2), BF16),
            pltpu.VMEM((14, TOK, QUARTER // 2), BF16),
            pltpu.VMEM((NZ, 8, TOK), F32),
            dma((14,)),
            dma((3,)),
            dma((4,)),
            dma((5,)),
            dma((4,)),
            dma((4,)),
            dma,
            dma((2,)),
            dma,
            dma((NZ,)),
            dma,
            dma((NZ,)),
            dma,
            dma,
            dma,
            dma((14,)),
            dma,
            dma,
        ],
        compiler_params=pltpu.CompilerParams(
            collective_id=0, has_side_effects=True, vmem_limit_bytes=60 << 20
        ),
        name="layer",
    )(
        memory_queries.T,
        memory_keys.T,
        memory_values.T,
        output_gate_preactivation.T,
        log_input_gate,
        forget_preactivation,
        head_forget_bias,
        forget_extra_boost,
        head_norm_gain.reshape(1, HW),
        memory_output_weight.reshape(NX, HW, D),
        residual,
        expert_norm_gain.reshape(1, D),
        routes.T,
        router_weight_matrix.T,
        routed_gate_weight,
        routed_up_weight,
        routed_down_weight,
        shared_gate_weight,
        shared_up_weight,
        shared_down_weight,
    )


def solution(mesh):
    split = Mesh(
        mesh.devices.reshape(NZ, NY, NC, mesh.shape["tp"]), ("sp_0", "sp_1", "sp_2", "tp")
    )
    return jax.shard_map(
        body,
        mesh=split,
        in_specs=(
            P(SP, "tp"),
            P(SP, "tp"),
            P(SP, "tp"),
            P(SP, "tp"),
            P("tp", SP),
            P("tp", SP),
            P("tp"),
            P("tp", SP),
            P("tp"),
            P(),
            P(SP, None),
            P(),
            P(SP, None),
            P(SP, None),
            P(SP, None, "tp"),
            P(SP, None, "tp"),
            P(SP, "tp", None),
            P(None, "tp"),
            P(None, "tp"),
            P("tp", None),
        ),
        out_specs=P(SP, "tp"),
        check_vma=False,
    )
```
